512 devices in a mesh: dp: 4 (over x), kv: 64 (over z, y), tp: 2 (over core).
Axes of the slice: x: 4, y: 8, z: 8, core: 2. Of those that a mesh axis runs over, the one named last changes fastest.
Arguments:
- tokens: bfloat16 [24, 4096], P('dp', 'kv'), may hold values from -64 to 64
- lengths: int32 [24], P('dp'), may hold values from 2048 to 16384, as said below
- attn_gain: float32 [4096], P('kv'), may hold values from 0.1 to 1.9
- query_weight: bfloat16 [4096, 4096], P('kv', 'tp'), may hold values from -0.09375 to 0.09375
- key_weight: bfloat16 [4096, 256], P('kv', 'tp'), may hold values from -0.1875 to 0.1875
- value_weight: bfloat16 [4096, 256], P('kv', 'tp'), may hold values from -0.09375 to 0.09375
- forget_weight: bfloat16 [4096, 4], replicated, may hold values from -0.25 to 0.25
- forget_offset: float32 [4], P('tp'), may hold values from -6 to 0
- cache_keys: bfloat16 [24, 16384, 256], P('dp', 'kv', 'tp'), may hold values from -1600 to 1600
- cache_values: bfloat16 [24, 16384, 256], P('dp', 'kv', 'tp'), may hold values from -6 to 6
- gate_sum: float32 [24, 4, 16384], P('dp', 'tp', 'kv'), may hold values from -1264 to 0
- out_weight: bfloat16 [4096, 4096], P('tp', 'kv'), may hold values from -0.1875 to 0.1875
- mlp_gain: float32 [4096], replicated, may hold values from 0.1 to 1.9
- up_weight: bfloat16 [4096, 16384], P(None, ('kv', 'tp')), may hold values from -0.09375 to 0.09375
- down_weight: bfloat16 [16384, 4096], P(('kv', 'tp')), may hold values from -0.1875 to 0.1875
Outputs:
- mixed: bfloat16 [24, 4096], P('dp', ('kv', 'tp'))
The draws below stay inside these ranges and needn't reach their ends.
Inputs may be any that keep to these rules, and one draw needn't show every extreme that they name: `lengths`: in every draw some sequence has all 16384 positions cached.
All inputs are finite; a program needn't handle non-finite values.
Results may differ from the reference program's by a relative error of at most 0.023.
Values may be sent and summed in bfloat16 or wider, within the bound.
No kernel may reach another device: no remote copies, remote signals or barrier semaphores. Data moves between devices by JAX's collectives and lax.ppermute only.
A program may use at most 64 MiB of HBM per device.

```python
import math
import jax
import jax.numpy as jnp
from jax import lax

D = 4096
HEADS = 64
HD = 64
KEY_VALUE_HEADS = 4
FF = 16384
CTX_DEV = 256
SEQUENCE_COUNT = 24
CTX = 16384
HEAD_GROUPS = 2


def seq_lengths(key):
    shorter = jax.random.randint(jax.random.fold_in(key, 11), (SEQUENCE_COUNT,), CTX // 8, CTX // 2 + 1)
    longer = jax.random.randint(jax.random.fold_in(key, 12), (SEQUENCE_COUNT,), CTX // 2, CTX + 1)
    shuffled = jax.random.permutation(jax.random.fold_in(key, 13), SEQUENCE_COUNT)
    ranking = jnp.argsort(shuffled)
    chosen = jnp.where(ranking < max(SEQUENCE_COUNT // 4, 1), longer, shorter)
    return jnp.where(ranking == 0, CTX, chosen).astype(jnp.int32)


def draw_lengths(key, part):
    return seq_lengths(key)


def draw_tokens(key, part):
    columns = jnp.arange(D, dtype=jnp.float32) / D - 0.5
    normal_draw = jnp.clip(jax.random.normal(jax.random.fold_in(key, 41), (SEQUENCE_COUNT, D), jnp.float32), -6.0, 6.0)
    column_scale = jnp.exp(math.log(10.0) * columns)
    row_factor = jnp.exp(jax.random.uniform(jax.random.fold_in(key, 42), (SEQUENCE_COUNT, 1), jnp.float32, -0.5 * math.log(10.0), 0.5 * math.log(10.0)))
    return (normal_draw * column_scale[None, :] * row_factor).astype(jnp.bfloat16)


def draw_gate_sum(key, part):
    lengths = seq_lengths(key)
    live_span = lengths.astype(jnp.float32)[:, None, None]
    token_offsets = jnp.arange(CTX)
    shuffled = jax.random.permutation(jax.random.fold_in(key, 21), KEY_VALUE_HEADS)
    slow_heads = (shuffled < KEY_VALUE_HEADS // 2)[None, :, None]
    blocks = CTX // CTX_DEV
    block_factor = jnp.exp(jax.random.uniform(jax.random.fold_in(key, 22), (SEQUENCE_COUNT, KEY_VALUE_HEADS, blocks), jnp.float32, -math.log(2.0), math.log(2.0)))
    block_factor = jnp.repeat(block_factor, CTX_DEV, axis=2)
    data_factor = jax.random.uniform(jax.random.fold_in(key, 23), (SEQUENCE_COUNT, KEY_VALUE_HEADS, CTX), jnp.float32, 0.5, 1.5)
    falloff_speeds = jnp.where(slow_heads, 0.5 / live_span, 1.0 / 40.0) * block_factor * data_factor
    spike_locations = jax.random.randint(jax.random.fold_in(key, 24), (SEQUENCE_COUNT, KEY_VALUE_HEADS, 3), 0, lengths[:, None, None])
    spike_penalty = jnp.log(1.0 - jax.random.uniform(jax.random.fold_in(key, 25), (SEQUENCE_COUNT, KEY_VALUE_HEADS, 3), jnp.float32, 0.2, 0.45))
    spike_events = jnp.sum(jnp.where(token_offsets[None, None, None, :] == spike_locations[..., None], spike_penalty[..., None], 0.0), axis=2)
    active_mask = token_offsets[None, None, :] < lengths[:, None, None]
    gate_logarithms = jnp.where(active_mask, spike_events - falloff_speeds, 0.0)
    return (jnp.sum(gate_logarithms, axis=2, keepdims=True) - jnp.cumsum(gate_logarithms, axis=2)).astype(jnp.float32)


def draw_cache_keys(key, part):
    drawn = 2.0 * jnp.clip(jax.random.normal(jax.random.fold_in(key, 31), (SEQUENCE_COUNT, CTX, KEY_VALUE_HEADS, HD), jnp.float32), -6.0, 6.0)
    return drawn.reshape(SEQUENCE_COUNT, CTX, KEY_VALUE_HEADS * HD).astype(jnp.bfloat16)


def spiked(result, rng, source, target, parts, factor):
    def block_of(dim):
        return (jnp.arange(result.shape[dim]) // (result.shape[dim] // parts)).reshape((-1,) + (1,) * (result.ndim - 1 - dim))

    one_side = jax.random.permutation(rng, parts)[block_of(target)]
    other_side = (block_of(target) + parts // 2) % parts
    return jnp.where((block_of(source) == one_side) | (block_of(source) == other_side), factor * result, result)


def steps_of(key, extent, cuts, low, high):
    def one(position, blocks):
        steps = jax.random.uniform(jax.random.fold_in(jax.random.fold_in(key, 6), position), (blocks,), jnp.float32, low / len(cuts), high / len(cuts))
        return jnp.repeat(jnp.exp(steps), extent[position] // blocks).reshape((-1,) + (1,) * (len(extent) - position - 1))

    level = one(*cuts[0])
    for cut in cuts[1:]:
        level = level * one(*cut)
    return level


def normal_values(key, shape, width, bound, cuts=(), held_as=jnp.bfloat16):
    values = width * jax.random.normal(key, shape, jnp.float32)
    if cuts:
        values = values * steps_of(key, shape, cuts, -0.22, 0.18)
    return jnp.clip(values, -bound, bound).astype(held_as)


def heavy_noise(rng, dims, deviation, reach, shards, heavy, kind=jnp.bfloat16):
    values = deviation * jax.random.normal(rng, dims, jnp.float32)
    if shards:
        values = values * steps_of(rng, dims, shards, -0.22, 0.18)
    return jnp.clip(spiked(values, jax.random.fold_in(rng, 3), *heavy), -reach, reach).astype(kind)


def setup_inputs(seed: int = 0) -> dict:
    arg_keys = jax.random.split(jax.random.key(seed), 16)
    return {
        "tokens": draw_tokens(jax.random.fold_in(arg_keys[15], 71), 0),
        "lengths": draw_lengths(jax.random.fold_in(arg_keys[15], 71), 0),
        "attn_gain": jnp.clip(1.0 + 0.18 * jax.random.normal(arg_keys[2], (D,), jnp.float32), 0.1, 1.9),
        "query_weight": normal_values(arg_keys[3], (D, HEADS * HD), D ** -0.5, 0.09375, ((0, 64), (1, 2))),
        "key_weight": normal_values(arg_keys[4], (D, KEY_VALUE_HEADS * HD), (D // 4) ** -0.5, 0.1875, ((0, 64), (1, 2))),
        "value_weight": normal_values(arg_keys[5], (D, KEY_VALUE_HEADS * HD), D ** -0.5, 0.09375, ((0, 64), (1, 2))),
        "forget_weight": normal_values(arg_keys[6], (D, KEY_VALUE_HEADS), (D // 8) ** -0.5, 0.25),
        "forget_offset": jnp.clip(-6.0 + 6.0 * jax.random.uniform(arg_keys[7], (KEY_VALUE_HEADS,), jnp.float32) ** steps_of(arg_keys[7], (KEY_VALUE_HEADS,), ((0, 2),), -0.2, 0.2), -6.0, 0.0),
        "cache_keys": draw_cache_keys(jax.random.fold_in(arg_keys[15], 71), 0),
        "cache_values": normal_values(arg_keys[9], (SEQUENCE_COUNT, CTX, KEY_VALUE_HEADS * HD), 1.0, 6.0, ((0, 4), (1, 64), (2, 2))),
        "gate_sum": draw_gate_sum(jax.random.fold_in(arg_keys[15], 71), 0),
        "out_weight": normal_values(arg_keys[11], (HEADS * HD, D), (D // 4) ** -0.5, 0.1875, ((0, 2), (1, 64))),
        "mlp_gain": jnp.clip(1.0 + 0.18 * jax.random.normal(arg_keys[12], (D,), jnp.float32), 0.1, 1.9),
        "up_weight": normal_values(arg_keys[13], (D, FF), D ** -0.5, 0.09375, ((1, 128),)),
        "down_weight": heavy_noise(arg_keys[14], (FF, D), FF ** -0.5, 0.1875, ((0, 128),), (0, 1, 128, 5.5)),
    }


epsilon = 1e-06

def reference(tokens, lengths, attn_gain, query_weight, key_weight, value_weight, forget_weight, forget_offset, cache_keys, cache_values, gate_sum, out_weight, mlp_gain, up_weight, down_weight):
    token_rows = tokens.astype(jnp.float32)
    row_scale = lax.rsqrt(lax.optimization_barrier(jnp.mean(token_rows * token_rows, axis=1, keepdims=True)) + epsilon)
    scaled_rows = (token_rows * attn_gain[None, :]).astype(jnp.bfloat16)
    queries = (jnp.dot(scaled_rows, query_weight, preferred_element_type=jnp.float32) * row_scale).astype(jnp.bfloat16)
    new_key = (jnp.dot(scaled_rows, key_weight, preferred_element_type=jnp.float32) * row_scale).astype(jnp.bfloat16)
    new_value = (jnp.dot(scaled_rows, value_weight, preferred_element_type=jnp.float32) * row_scale).astype(jnp.bfloat16)
    log_forget = jax.nn.log_sigmoid(jnp.dot(scaled_rows, forget_weight, preferred_element_type=jnp.float32) * row_scale + forget_offset[None, :])
    group_size = HEADS // KEY_VALUE_HEADS
    score_scale = HD ** (-0.5)
    token_offsets = jnp.arange(CTX)

    def one_sequence(inputs_one):
        query_row, key_rows, value_rows, gates, length, forget_row, own_key, own_value = inputs_one
        query_heads = query_row.astype(jnp.float32).reshape(KEY_VALUE_HEADS, group_size, HD)
        key_heads = key_rows.astype(jnp.float32).reshape(CTX, KEY_VALUE_HEADS, HD)
        value_heads = value_rows.astype(jnp.float32).reshape(CTX, KEY_VALUE_HEADS, HD)
        scores = jnp.einsum('kgd,pkd->kgp', query_heads, key_heads) * score_scale
        scores = scores + gates[:, None, :] + forget_row[:, None, None]
        active_mask = token_offsets < length
        scores = jnp.where(active_mask[None, None, :], scores, -jnp.inf)
        own_score = jnp.einsum('kgd,kd->kg', query_heads, own_key.astype(jnp.float32).reshape(KEY_VALUE_HEADS, HD)) * score_scale
        row_top = jnp.maximum(lax.optimization_barrier(jnp.max(scores, axis=2)), own_score)
        weight = jnp.exp(scores - row_top[..., None])
        own_weight = jnp.exp(own_score - row_top)
        totals = lax.optimization_barrier(jnp.sum(weight, axis=2)) + own_weight
        rounded = lax.optimization_barrier(weight.astype(jnp.bfloat16)).astype(jnp.float32)
        own_rounded = lax.optimization_barrier(own_weight.astype(jnp.bfloat16)).astype(jnp.float32)
        summed = jnp.einsum('kgp,pkd->kgd', rounded, value_heads)
        summed = summed + own_rounded[..., None] * own_value.astype(jnp.float32).reshape(KEY_VALUE_HEADS, 1, HD)
        return (summed / totals[..., None]).reshape(HEADS * HD).astype(jnp.bfloat16)
    attended = lax.map(one_sequence, (queries, cache_keys, cache_values, gate_sum, lengths, log_forget, new_key, new_value))
    group_width = HEADS * HD // HEAD_GROUPS
    summed_mid = token_rows
    for group_index in range(HEAD_GROUPS):
        partial_value = jnp.dot(attended[:, group_index * group_width:(group_index + 1) * group_width], out_weight[group_index * group_width:(group_index + 1) * group_width], preferred_element_type=jnp.float32)
        partial_value = lax.optimization_barrier(partial_value.astype(jnp.bfloat16)).astype(jnp.float32)
        summed_mid = summed_mid + partial_value
    mid_rows = summed_mid.astype(jnp.bfloat16)
    mid_wide = mid_rows.astype(jnp.float32)
    normed_mid = (mid_wide * mlp_gain[None, :] * lax.rsqrt(lax.optimization_barrier(jnp.mean(mid_wide * mid_wide, axis=1, keepdims=True)) + epsilon)).astype(jnp.bfloat16)
    hidden = jnp.square(jax.nn.relu(jnp.dot(normed_mid, up_weight, preferred_element_type=jnp.float32))).astype(jnp.bfloat16)
    return (mid_wide + jnp.dot(hidden, down_weight, preferred_element_type=jnp.float32)).astype(jnp.bfloat16)
```

```python
import functools

import jax
import jax.numpy as jnp
from jax import lax
from jax.sharding import Mesh
from jax.sharding import PartitionSpec as P

D = 4096
HEADS = 64
HD = 64
KEY_VALUE_HEADS = 4
KV = ("kv_0", "kv_1")
KV_TP = ("kv_0", "kv_1", "tp")


epsilon = 1e-06
floor_score = -1e30


def over_pieces(x, axis):
    pieces = lax.all_gather(x, axis).astype(jnp.float32)
    return pieces.sum(axis=0)


def from_everyone(x, axis):
    copies = jnp.broadcast_to(x, (lax.axis_size(axis), *x.shape))
    return lax.all_to_all(copies, axis, split_axis=0, concat_axis=0, tiled=True)


def in_order(pieces, dim):
    pieces = jnp.moveaxis(pieces, 0, dim)
    dims = pieces.shape
    return pieces.reshape(*dims[:dim], dims[dim] * dims[dim + 1], *dims[dim + 2 :])


def gathered_copies(x, axis, dim):
    pieces = from_everyone(x, axis)
    return in_order(pieces, dim)


def cut_along(x, dim, devices):
    dims = x.shape
    pieces = x.reshape(*dims[:dim], devices, dims[dim] // devices, *dims[dim + 1 :])
    return jnp.moveaxis(pieces, dim, 0)


def sent_and_summed(x, axis, dim):
    devices = lax.axis_size(axis)
    pieces = lax.all_to_all(cut_along(x, dim, devices), axis, 0, 0, tiled=True)
    return jnp.sum(pieces.astype(jnp.float32), axis=0)


def summed_everywhere(x):
    for axis in ("kv_1", "kv_0"):
        x = from_everyone(x.astype(jnp.bfloat16), axis).astype(jnp.float32).sum(axis=0)
    return x


def combined_everywhere(top, total, values):
    rows, heads = top.shape
    for axis in ("kv_1", "kv_0"):
        line = jnp.concatenate((values, top, total), axis=1).astype(jnp.bfloat16)
        pieces = from_everyone(line, axis).astype(jnp.float32)
        values = pieces[:, :, : heads * HD]
        top = pieces[:, :, heads * HD : heads * (HD + 1)]
        total = pieces[:, :, heads * (HD + 1) :]
        merged = top.max(axis=0)
        scale = jnp.exp(top - merged[None])
        total = (total * scale).sum(axis=0)
        wide = jnp.repeat(scale, HD, axis=2)
        values = (values * wide).sum(axis=0)
        top = merged
    return top, total, values


def shards(
    tokens,
    lengths,
    attn_gain,
    query_weight,
    key_weight,
    value_weight,
    forget_weight,
    forget_offset,
    cache_keys,
    cache_values,
    gate_sum,
    out_weight,
    mlp_gain,
    up_weight,
    down_weight,
):
    row_count = tokens.shape[0]
    feature_cols = tokens.shape[1]
    kv_place = lax.axis_index(KV)
    tp_place = lax.axis_index("tp")
    local_heads = key_weight.shape[1] // HD
    group_size = HEADS // KEY_VALUE_HEADS
    token_rows = tokens.astype(jnp.float32)
    scaled_rows = (token_rows * attn_gain[None, :]).astype(jnp.bfloat16)
    square_part = jnp.sum(token_rows * token_rows, axis=1)
    query_part = jnp.dot(scaled_rows, query_weight, preferred_element_type=jnp.float32)
    key_part = jnp.dot(scaled_rows, key_weight, preferred_element_type=jnp.float32)
    value_part = jnp.dot(scaled_rows, value_weight, preferred_element_type=jnp.float32)
    gate_rows = lax.dynamic_slice(
        forget_weight,
        (kv_place * feature_cols, tp_place * local_heads),
        (feature_cols, local_heads),
    )
    forget_part = jnp.dot(scaled_rows, gate_rows, preferred_element_type=jnp.float32)
    widths = (query_part.shape[1], key_part.shape[1], value_part.shape[1], forget_part.shape[1])
    parts = jnp.concatenate(
        (query_part, key_part, value_part, forget_part, square_part[:, None]), axis=1
    )
    sums = summed_everywhere(parts)
    query_sum = sums[:, : widths[0]]
    key_sum = sums[:, widths[0] : widths[0] + widths[1]]
    value_sum = sums[:, widths[0] + widths[1] : sum(widths[:3])]
    forget_sum = sums[:, sum(widths[:3]) : sum(widths)]
    square_sum = sums[:, sum(widths)]
    row_scale = lax.rsqrt(square_sum / D + epsilon)[:, None]
    queries = (query_sum * row_scale).astype(jnp.bfloat16)
    new_key = (key_sum * row_scale).astype(jnp.bfloat16)
    new_value = (value_sum * row_scale).astype(jnp.bfloat16)
    log_forget = jax.nn.log_sigmoid(forget_sum * row_scale + forget_offset[None, :])
    positions_here = cache_keys.shape[1]
    key_heads = cache_keys.reshape(row_count, positions_here, local_heads, HD)
    value_heads = cache_values.reshape(row_count, positions_here, local_heads, HD)
    query_heads = queries.reshape(row_count, local_heads, group_size, HD)
    scores = jnp.einsum(
        "skgd,spkd->skgp", query_heads, key_heads, preferred_element_type=jnp.float32
    ) * HD ** (-0.5)
    scores = scores + gate_sum[:, :, None, :] + log_forget[:, :, None, None]
    cache_pos = kv_place * positions_here + jnp.arange(positions_here)
    active_mask = (cache_pos[None, :] < lengths[:, None])[:, None, None, :]
    local_top = jnp.max(jnp.where(active_mask, scores, floor_score), axis=3)
    local_top = local_top.astype(jnp.bfloat16).astype(jnp.float32)
    weights = jnp.where(active_mask, jnp.exp(scores - local_top[..., None]), 0.0)
    local_total = jnp.sum(weights, axis=3)
    local_values = jnp.einsum(
        "skgp,spkd->skgd",
        weights.astype(jnp.bfloat16),
        value_heads,
        preferred_element_type=jnp.float32,
    )
    head_cols = local_heads * group_size
    merged_top, merged_total, merged_values = combined_everywhere(
        local_top.reshape(row_count, head_cols),
        local_total.reshape(row_count, head_cols),
        local_values.reshape(row_count, head_cols * HD),
    )
    own_score = jnp.einsum(
        "skgd,skd->skg",
        query_heads,
        new_key.reshape(row_count, local_heads, HD),
        preferred_element_type=jnp.float32,
    ).reshape(row_count, head_cols) * HD ** (-0.5)
    final_top = jnp.maximum(merged_top, own_score)
    past_scale = jnp.exp(merged_top - final_top)
    own_weight = jnp.exp(own_score - final_top)
    totals = merged_total * past_scale + own_weight
    own_rounded = lax.optimization_barrier(own_weight.astype(jnp.bfloat16)).astype(jnp.float32)
    own_values = jnp.broadcast_to(
        new_value.astype(jnp.float32).reshape(row_count, local_heads, 1, HD),
        (row_count, local_heads, group_size, HD),
    ).reshape(row_count, head_cols * HD)
    weighted = (
        merged_values * jnp.repeat(past_scale, HD, axis=1)
        + jnp.repeat(own_rounded, HD, axis=1) * own_values
    )
    attended = (weighted / jnp.repeat(totals, HD, axis=1)).astype(jnp.bfloat16)
    partial_out = jnp.dot(attended, out_weight, preferred_element_type=jnp.float32)
    head_sum = over_pieces(partial_out.astype(jnp.bfloat16), "tp").astype(jnp.float32)
    mid_cols = (token_rows + head_sum).astype(jnp.bfloat16)
    mid_rows = gathered_copies(mid_cols, KV, 1)
    mid_wide = mid_rows.astype(jnp.float32)
    normed_mid = (
        mid_wide
        * mlp_gain[None, :]
        * lax.rsqrt(jnp.mean(mid_wide * mid_wide, axis=1, keepdims=True) + epsilon)
    ).astype(jnp.bfloat16)
    hidden = jnp.square(
        jax.nn.relu(jnp.dot(normed_mid, up_weight, preferred_element_type=jnp.float32))
    ).astype(jnp.bfloat16)
    mixer_term = jnp.dot(hidden, down_weight, preferred_element_type=jnp.float32)
    kv_count = lax.axis_size(KV)
    tp_count = lax.axis_size("tp")
    pair_sum = over_pieces(mixer_term.astype(jnp.bfloat16), "tp")
    pair_cols = sent_and_summed(pair_sum.astype(jnp.bfloat16), KV, 1)
    out_width = pair_cols.shape[1] // tp_count
    mixer_share = lax.dynamic_slice_in_dim(pair_cols, tp_place * out_width, out_width, 1)
    out_cols = mixer_share.shape[1]
    start_col = (kv_place * tp_count + tp_place) * out_cols
    mid_share = lax.dynamic_slice_in_dim(mid_wide, start_col, out_cols, 1)
    return (mid_share + mixer_share).astype(jnp.bfloat16)


def solution(mesh):
    torus = Mesh(
        mesh.devices.reshape(mesh.shape["dp"], 8, 8, mesh.shape["tp"]), ("dp", "kv_0", "kv_1", "tp")
    )
    placed = (
        P("dp", KV),
        P("dp"),
        P(KV),
        P(KV, "tp"),
        P(KV, "tp"),
        P(KV, "tp"),
        P(),
        P("tp"),
        P("dp", KV, "tp"),
        P("dp", KV, "tp"),
        P("dp", "tp", KV),
        P("tp", KV),
        P(),
        P(None, KV_TP),
        P(KV_TP, None),
    )
    return jax.shard_map(
        shards, mesh=torus, in_specs=placed, out_specs=P("dp", KV_TP), check_vma=False
    )
```

```python
import functools

import jax
import jax.numpy as jnp
from jax import lax
from jax.experimental import pallas as pl
from jax.experimental.pallas import tpu as pltpu
from jax.sharding import Mesh
from jax.sharding import PartitionSpec as P

D = 4096
HEADS = 64
HD = 64
KEY_VALUE_HEADS = 4
KV = ("kv_0", "kv_1")
KV_TP = ("kv_0", "kv_1", "tp")
LANES = 128
HALF = 64
RING = 8

epsilon = 1e-06
floor_score = -1e30

VMEM = pl.BlockSpec(memory_space=pltpu.VMEM)
SMEM = pl.BlockSpec(memory_space=pltpu.SMEM)


def call(body, out_shape, in_specs, scratch=(), flops=1 << 20):
    return pl.pallas_call(
        body,
        out_shape=out_shape,
        in_specs=in_specs,
        out_specs=jax.tree.map(lambda _: VMEM, out_shape),
        scratch_shapes=scratch,
        compiler_params=pltpu.CompilerParams(vmem_limit_bytes=16 << 20),
        cost_estimate=pl.CostEstimate(flops=flops, bytes_accessed=1 << 20, transcendentals=0),
    )


def lanes_of(shape):
    return lax.broadcasted_iota(jnp.int32, shape, len(shape) - 1)


def rounded(x):
    return x.astype(jnp.bfloat16).astype(jnp.float32)


def exchanged(x, axes):
    return lax.all_to_all(x, axes, split_axis=0, concat_axis=0, tiled=True)


def dotted(a, b, b_dim=0):
    return lax.dot_general(
        a, b, (((1,), (b_dim,)), ((), ())), preferred_element_type=jnp.float32
    )


def project(place, tokens, gain, query_w, key_w, value_w, forget_w, out):
    rows = tokens[...].astype(jnp.float32)
    scaled = (rows * gain[...]).astype(jnp.bfloat16)
    wide = scaled.astype(jnp.float32)
    gates = forget_w[...].astype(jnp.float32)
    square = jnp.sum(rows * rows, axis=1, keepdims=True)
    square_high = rounded(square)
    columns = [
        jnp.sum(wide * gates[n : n + 1, :], axis=1, keepdims=True) for n in range(gates.shape[0])
    ] + [square_high, square - square_high]
    lane = lanes_of((rows.shape[0], LANES))
    extra = jnp.zeros(lane.shape, jnp.float32)
    for n, column in enumerate(columns):
        extra = jnp.where(lane == n, column, extra)
    line = jnp.concatenate(
        (
            dotted(scaled, query_w[...]),
            dotted(scaled, key_w[...]),
            dotted(scaled, value_w[...]),
            extra,
        ),
        axis=1,
    ).astype(jnp.bfloat16)
    for k in range(RING):
        out[k] = line


def summed(parts):
    total = parts[0].astype(jnp.float32)
    for k in range(1, RING):
        total = total + parts[k].astype(jnp.float32)
    return total


def resend(parts, out):
    line = summed(parts).astype(jnp.bfloat16)
    for k in range(RING):
        out[k] = line


def attend(place, lengths, offsets, parts, keys, values, gate, out, turned):
    count, positions = keys.shape[0], keys.shape[1]
    pairs = turned.shape[0] // 8
    spot, core = place[0], place[1]
    line = summed(parts)
    width = pairs * LANES
    extra = line[:, width + 2 * LANES :]
    row_scale = lax.rsqrt((extra[:, 4:5] + extra[:, 5:6]) / D + epsilon)
    ready = rounded(line[:, : width + 2 * LANES] * row_scale)
    new_key = ready[:, width : width + LANES]
    new_value = ready[:, width + LANES :]
    forget = []
    for n in range(2):
        gate_in = jnp.where(core == 0, extra[:, n : n + 1], extra[:, n + 2 : n + 3])
        z = gate_in * row_scale + offsets[n]
        forget.append(jnp.minimum(z, 0.0) - jnp.log1p(jnp.exp(-jnp.abs(z))))
    for j in range(pairs):
        turned[8 * j : 8 * j + count, :] = ready[:, LANES * j : LANES * (j + 1)]
    lane = lanes_of((pairs, LANES))
    row = lax.broadcasted_iota(jnp.int32, (pairs, LANES), 0)
    straight = (lane < HALF) == (row < pairs // 2)
    first = spot == 0
    place_of = spot * positions + lanes_of((1, positions))
    stat_lane = lanes_of((8, LANES))
    stats = jnp.zeros((8, LANES), jnp.float32)
    blocks = []
    for s in range(count):
        both = turned[pl.ds(s, pairs, stride=8), :]
        query = jnp.concatenate(
            (
                jnp.where(straight, both, 0.0),
                jnp.where(straight, pltpu.roll(both, HALF, 1), 0.0),
            ),
            axis=0,
        )
        score = dotted(query.astype(jnp.bfloat16), keys[s], 1) * HD ** (-0.5)
        lines = [
            jnp.broadcast_to(gate[s, n : n + 1, :] + forget[n][s : s + 1, :], (8, positions))
            for n in range(2)
        ]
        live = place_of < lengths[s]
        score = jnp.where(live, score + jnp.concatenate(lines + lines, axis=0), floor_score)
        own = jnp.sum(query * new_key[s : s + 1, :], axis=1, keepdims=True) * HD ** (-0.5)
        own = jnp.where(first, own, floor_score)
        top = rounded(jnp.maximum(jnp.max(score, axis=1, keepdims=True), own))
        weight = jnp.where(live, jnp.exp(score - top), 0.0)
        own_weight = jnp.where(first, jnp.exp(own - top), 0.0)
        total = jnp.sum(weight, axis=1, keepdims=True) + own_weight
        mixed = dotted(weight.astype(jnp.bfloat16), values[s])
        mixed = mixed + rounded(own_weight) * new_value[s : s + 1, :]
        blocks.append(
            jnp.where(straight, mixed[:pairs], pltpu.roll(mixed[pairs:], HALF, 1)).astype(
                jnp.bfloat16
            )
        )
        total_high = rounded(total)
        for n, column in enumerate((top, total_high, total - total_high)):
            for g in range(4):
                stats = jnp.where(
                    stat_lane == 32 * g + 8 * n + s, column[8 * g : 8 * g + 8], stats
                )
    blocks.append(stats.astype(jnp.bfloat16))
    line = jnp.concatenate(blocks, axis=0)
    for k in range(RING):
        out[k] = line


def spread(compact, block, low):
    s, half = divmod(block, 2)
    left, right = (s, 64 + s) if half == 0 else (96 + s, 32 + s)
    return jnp.where(low, compact[:, left : left + 1], compact[:, right : right + 1])


def merged(parts):
    rows = parts.shape[1]
    blocks = rows // 8 - 1
    stats = [parts[k, rows - 8 : rows, :].astype(jnp.float32) for k in range(RING)]
    top = functools.reduce(jnp.maximum, stats)
    scales = [jnp.exp(x - top) for x in stats]
    total = functools.reduce(
        jnp.add,
        [
            scale * (pltpu.roll(x, LANES - 8, 1) + pltpu.roll(x, LANES - 16, 1))
            for scale, x in zip(scales, stats)
        ],
    )
    low = lanes_of((8, LANES)) < HALF
    mixed = []
    for b in range(blocks):
        acc = jnp.zeros((8, LANES), jnp.float32)
        for k in range(RING):
            acc = acc + parts[k, 8 * b : 8 * b + 8, :].astype(jnp.float32) * spread(
                scales[k], b, low
            )
        mixed.append(acc)
    return top, total, mixed, low


def combine(parts, out):
    top, total, mixed, _ = merged(parts)
    kind = lanes_of((8, LANES)) % 32
    total_high = rounded(total)
    stats = jnp.where(
        kind < 8,
        top,
        jnp.where(
            kind < 16, pltpu.roll(total_high, 8, 1), pltpu.roll(total - total_high, 16, 1)
        ),
    )
    line = jnp.concatenate([x.astype(jnp.bfloat16) for x in mixed + [stats]], axis=0)
    for k in range(RING):
        out[k] = line


def finish(place, parts, tokens, out_w, out, turned):
    _, total, mixed, low = merged(parts)
    inverse = 1.0 / total
    for b, acc in enumerate(mixed):
        turned[8 * b : 8 * b + 8, :] = rounded(acc * spread(inverse, b, low))
    count = tokens.shape[0]
    pairs = turned.shape[0] // count
    attended = jnp.concatenate(
        [turned[pl.ds(j, count, stride=pairs), :] for j in range(pairs)], axis=1
    ).astype(jnp.bfloat16)
    part = dotted(attended, out_w[...], 1)
    part = part + jnp.where(place[1] == 0, tokens[...].astype(jnp.float32), 0.0)
    third = count // 2
    piece = jnp.concatenate((part[:third], part[third:]), axis=1).astype(jnp.bfloat16)
    for k in range(out.shape[0]):
        out[k] = piece


def mix(parts, gain, up_w, down_w, mid_out, out, mid):
    count, width = mid.shape
    third = count // 2
    low = lanes_of((third, LANES)) < HALF
    square = jnp.zeros((count, LANES), jnp.float32)
    for t in range(width // LANES):
        a = rounded(
            parts[4 * t].astype(jnp.float32) + parts[4 * t + 1].astype(jnp.float32)
        )
        b = rounded(
            parts[4 * t + 2].astype(jnp.float32) + parts[4 * t + 3].astype(jnp.float32)
        )
        at = slice(LANES * t, LANES * (t + 1))
        mid[:third, at] = jnp.where(low, a, pltpu.roll(b, HALF, 1))
        mid[third:, at] = jnp.where(low, pltpu.roll(a, HALF, 1), b)
        tile = mid[:, at]
        square = square + tile * tile
    scale = lax.rsqrt(jnp.sum(square, axis=1, keepdims=True) / D + epsilon)
    rows = mid[...]
    mid_out[...] = rows.astype(jnp.bfloat16)
    normed = (rows * gain[...] * scale).astype(jnp.bfloat16)
    hidden = jnp.square(jnp.maximum(dotted(normed, up_w[...]), 0.0))
    hidden = jnp.concatenate((hidden, jnp.zeros((8 - count, LANES), jnp.float32)), axis=0)
    picked = jnp.concatenate(
        [
            hidden[4 * a + (u + k) % 4 : 4 * a + (u + k) % 4 + 1]
            for k in range(4)
            for u in range(4)
            for a in range(2)
        ],
        axis=0,
    ).astype(jnp.bfloat16)
    spread_out = dotted(picked, down_w[...])
    group = lanes_of((8, LANES)) // 32
    owner = lax.broadcasted_iota(jnp.int32, (8, LANES), 0) // 2
    turn = (group - owner) % 4
    for t in range(width // LANES):
        at = slice(LANES * t, LANES * (t + 1))
        tile = spread_out[:8, at]
        for k in range(1, 4):
            tile = jnp.where(
                turn == k, pltpu.roll(spread_out[8 * k : 8 * k + 8, at], 32 * k, 1), tile
            )
        out[8 * t : 8 * t + 8, :] = tile.astype(jnp.bfloat16)


def close(place, parts, mid, out):
    total = jnp.zeros((8, LANES), jnp.float32)
    for t in range(parts.shape[0] // 8):
        total = total + parts[8 * t : 8 * t + 8, :].astype(jnp.float32)
    pair = total[0:2] + total[2:4] + total[4:6] + total[6:8]
    count, width = out.shape
    number = place[0] * 2 + place[1]
    tile = mid[:, pl.ds(pl.multiple_of((number // 4) * LANES, LANES), LANES)]
    group = number % 4
    own = jnp.zeros((count, width), jnp.float32)
    for n in range(4):
        own = jnp.where(
            group == n, tile[:, width * n : width * (n + 1)].astype(jnp.float32), own
        )
    rows = [pair[r // 4 : r // 4 + 1, 32 * (r % 4) : 32 * (r % 4) + 32] for r in range(count)]
    out[...] = (own + jnp.concatenate(rows, axis=0)).astype(jnp.bfloat16)


def shards(
    tokens,
    lengths,
    attn_gain,
    query_weight,
    key_weight,
    value_weight,
    forget_weight,
    forget_offset,
    cache_keys,
    cache_values,
    gate_sum,
    out_weight,
    mlp_gain,
    up_weight,
    down_weight,
):
    rows, cols = tokens.shape
    spot = lax.axis_index(KV)
    place = jnp.stack((spot, lax.axis_index("tp"))).astype(jnp.int32)
    bf16 = functools.partial(jax.ShapeDtypeStruct, dtype=jnp.bfloat16)
    heads_wide = query_weight.shape[1]
    line = heads_wide + 3 * LANES
    gates = lax.dynamic_slice(
        forget_weight.T, (0, spot * cols), (forget_weight.shape[1], cols)
    )
    x = call(project, bf16((RING, rows, line)), [SMEM] + [VMEM] * 6)(
        place, tokens, attn_gain[None, :], query_weight, key_weight, value_weight, gates
    )
    x = exchanged(x, "kv_1")
    x = call(resend, bf16((RING, rows, line)), [VMEM])(x)
    x = exchanged(x, "kv_0")
    stack = rows * heads_wide // LANES
    packed = stack + 8
    x = call(
        attend,
        bf16((RING, packed, LANES)),
        [SMEM] * 3 + [VMEM] * 4,
        [pltpu.VMEM((8 * heads_wide // LANES, LANES), jnp.float32)],
    )(place, lengths, forget_offset, x, cache_keys, cache_values, gate_sum)
    x = exchanged(x, "kv_1")
    x = call(combine, bf16((RING, packed, LANES)), [VMEM])(x)
    x = exchanged(x, "kv_0")
    group = lax.axis_size(KV_TP)
    x = call(
        finish,
        bf16((group, rows // 2, LANES)),
        [SMEM] + [VMEM] * 3,
        [pltpu.VMEM((stack, LANES), jnp.float32)],
    )(place, x, tokens, out_weight.T)
    x = exchanged(x, KV_TP)
    mid, x = call(
        mix,
        (bf16((rows, D)), bf16((2 * group, LANES))),
        [VMEM] * 4,
        [pltpu.VMEM((rows, D), jnp.float32)],
    )(x, mlp_gain[None, :], up_weight, down_weight)
    x = exchanged(x.reshape(group, 2, LANES), KV_TP).reshape(2 * group, LANES)
    return call(close, bf16((rows, D // group)), [SMEM, VMEM, VMEM])(place, x, mid)


def solution(mesh):
    torus = Mesh(
        mesh.devices.reshape(mesh.shape["dp"], 8, 8, mesh.shape["tp"]), ("dp", "kv_0", "kv_1", "tp")
    )
    placed = (
        P("dp", KV),
        P("dp"),
        P(KV),
        P(KV, "tp"),
        P(KV, "tp"),
        P(KV, "tp"),
        P(),
        P("tp"),
        P("dp", KV, "tp"),
        P("dp", KV, "tp"),
        P("dp", "tp", KV),
        P("tp", KV),
        P(),
        P(None, KV_TP),
        P(KV_TP, None),
    )
    return jax.shard_map(
        shards, mesh=torus, in_specs=placed, out_specs=P("dp", KV_TP), check_vma=False
    )
```

```python
import functools

import jax
import jax.numpy as jnp
from jax import lax
from jax.experimental import pallas as pl
from jax.experimental.pallas import tpu as pltpu
from jax.sharding import Mesh
from jax.sharding import PartitionSpec as P

D = 4096
HEADS = 64
HD = 64
KEY_VALUE_HEADS = 4
KV = ("kv_0", "kv_1")
KV_TP = ("kv_0", "kv_1", "tp")
LANES = 128
HALF = 64
RING = 8

epsilon = 1e-06
floor_score = -1e30

VMEM = pl.BlockSpec(memory_space=pltpu.VMEM)
HBM = pl.BlockSpec(memory_space=pltpu.HBM)


def call(body, out_shape, in_specs, scratch=(), flops=1 << 20):
    return pl.pallas_call(
        body,
        out_shape=out_shape,
        in_specs=in_specs,
        out_specs=jax.tree.map(lambda _: VMEM, out_shape),
        scratch_shapes=scratch,
        compiler_params=pltpu.CompilerParams(vmem_limit_bytes=16 << 20),
        cost_estimate=pl.CostEstimate(flops=flops, bytes_accessed=1 << 20, transcendentals=0),
    )


def lanes_of(shape):
    return lax.broadcasted_iota(jnp.int32, shape, len(shape) - 1)


def rounded(x):
    return x.astype(jnp.bfloat16).astype(jnp.float32)


def exchanged(x, axes):
    return lax.all_to_all(x, axes, split_axis=0, concat_axis=0, tiled=True)


def dotted(a, b, b_dim=0):
    return lax.dot_general(
        a, b, (((1,), (b_dim,)), ((), ())), preferred_element_type=jnp.float32
    )


def kv_spot():
    return lax.axis_index("kv_0") * lax.axis_size("kv_1") + lax.axis_index("kv_1")


def project(
    tokens_far, gain_far, query_far, key_far, value_far, forget_far, out,
    tokens, gain, query_w, key_w, value_w, forget_w, dense, arrived,
):
    spot = kv_spot()
    window = pl.ds(pl.multiple_of((spot // 2) * LANES, LANES), LANES)
    copies = [
        pltpu.make_async_copy(far, near, arrived.at[n])
        for n, (far, near) in enumerate(
            (
                (query_far, query_w),
                (tokens_far, tokens),
                (gain_far, gain),
                (key_far, key_w),
                (value_far, value_w),
                (forget_far.at[:, window], forget_w),
            )
        )
    ]
    for copy in copies:
        copy.start()
    for copy in copies[1:3]:
        copy.wait()
    rows = tokens[...].astype(jnp.float32)
    count, cols = rows.shape
    scaled = (rows * gain[...]).astype(jnp.bfloat16)
    wide = scaled.astype(jnp.float32)
    square = jnp.sum(rows * rows, axis=1, keepdims=True)
    square_high = rounded(square)
    for copy in copies[3:]:
        copy.wait()
    gates = forget_w[...].astype(jnp.float32)
    gates = jnp.where(spot % 2 == 0, gates[:, :cols], gates[:, cols:])
    columns = [
        jnp.sum(wide * gates[n : n + 1, :], axis=1, keepdims=True) for n in range(gates.shape[0])
    ] + [square_high, square - square_high]
    lane = lanes_of((count, LANES))
    extra = jnp.zeros(lane.shape, jnp.float32)
    for n, column in enumerate(columns):
        extra = jnp.where((lane == n) | (lane == n + HALF), column, extra)
    third = count // 2
    extra = jnp.where(lane[:third] < HALF, extra[:third], extra[third:])
    copies[0].wait()
    query = dotted(scaled, query_w[...])
    pairs = query.shape[1] // LANES
    stack = pairs * count
    for j in range(pairs):
        dense[pl.ds(j, count, stride=pairs), :] = query[:, LANES * j : LANES * (j + 1)]
    dense[stack : stack + count, :] = dotted(scaled, key_w[...])
    dense[stack + count : stack + 2 * count, :] = dotted(scaled, value_w[...])
    dense[stack + 2 * count : stack + 2 * count + third, :] = extra
    spare = stack + 2 * count + third
    dense[spare:, :] = jnp.zeros((dense.shape[0] - spare, LANES), jnp.float32)
    line = dense[...].astype(jnp.bfloat16)
    for k in range(RING):
        out[k] = line


def summed(parts):
    total = parts[0].astype(jnp.float32)
    for k in range(1, RING):
        total = total + parts[k].astype(jnp.float32)
    return total


def resend(parts, out):
    line = summed(parts).astype(jnp.bfloat16)
    for k in range(RING):
        out[k] = line


def attend(lengths, offsets, parts, keys, values, gate, out):
    count, positions = keys.shape[0], keys.shape[1]
    spot = kv_spot()
    line = summed(parts)
    stack = line.shape[0] - 16
    pairs = stack // count
    tail = line[stack:]
    extra = tail[2 * count : 2 * count + count // 2]
    extra = jnp.concatenate((extra, pltpu.roll(extra, HALF, 1)), axis=0)
    row_scale = lax.rsqrt((extra[:, 4:5] + extra[:, 5:6]) / D + epsilon)
    new_key = rounded(tail[:count] * row_scale)
    new_value = rounded(tail[count : 2 * count] * row_scale)
    forget = []
    for n in range(2):
        gate_in = jnp.where(
            lax.axis_index("tp") == 0, extra[:, n : n + 1], extra[:, n + 2 : n + 3]
        )
        z = gate_in * row_scale + offsets[:, n : n + 1]
        forget.append(jnp.minimum(z, 0.0) - jnp.log1p(jnp.exp(-jnp.abs(z))))
    lane = lanes_of((pairs, LANES))
    row = lax.broadcasted_iota(jnp.int32, (pairs, LANES), 0)
    straight = (lane < HALF) == (row < pairs // 2)
    first = spot == 0
    place_of = spot * positions + lanes_of((1, positions))
    stat_lane = lanes_of((8, LANES))
    stats = jnp.zeros((8, LANES), jnp.float32)
    blocks = []
    for s in range(count):
        both = rounded(line[pairs * s : pairs * (s + 1)] * row_scale[s : s + 1, :])
        query = jnp.concatenate(
            (
                jnp.where(straight, both, 0.0),
                jnp.where(straight, pltpu.roll(both, HALF, 1), 0.0),
            ),
            axis=0,
        )
        score = dotted(query.astype(jnp.bfloat16), keys[s], 1) * HD ** (-0.5)
        lines = [
            jnp.broadcast_to(gate[s, n : n + 1, :] + forget[n][s : s + 1, :], (8, positions))
            for n in range(2)
        ]
        live = place_of < lengths[:, s : s + 1]
        score = jnp.where(live, score + jnp.concatenate(lines + lines, axis=0), floor_score)
        own = jnp.sum(query * new_key[s : s + 1, :], axis=1, keepdims=True) * HD ** (-0.5)
        own = jnp.where(first, own, floor_score)
        top = rounded(jnp.maximum(jnp.max(score, axis=1, keepdims=True), own))
        weight = jnp.where(live, jnp.exp(score - top), 0.0)
        own_weight = jnp.where(first, jnp.exp(own - top), 0.0)
        total = jnp.sum(weight, axis=1, keepdims=True) + own_weight
        mixed = dotted(weight.astype(jnp.bfloat16), values[s])
        mixed = mixed + rounded(own_weight) * new_value[s : s + 1, :]
        blocks.append(
            jnp.where(straight, mixed[:pairs], pltpu.roll(mixed[pairs:], HALF, 1)).astype(
                jnp.bfloat16
            )
        )
        total_high = rounded(total)
        for n, column in enumerate((top, total_high, total - total_high)):
            for g in range(4):
                stats = jnp.where(
                    stat_lane == 32 * g + 8 * n + s, column[8 * g : 8 * g + 8], stats
                )
    blocks.append(stats.astype(jnp.bfloat16))
    line = jnp.concatenate(blocks, axis=0)
    for k in range(RING):
        out[k] = line


def spread(compact, block, low):
    s, half = divmod(block, 2)
    left, right = (s, 64 + s) if half == 0 else (96 + s, 32 + s)
    return jnp.where(low, compact[:, left : left + 1], compact[:, right : right + 1])


def merged(parts):
    rows = parts.shape[1]
    blocks = rows // 8 - 1
    stats = [parts[k, rows - 8 : rows, :].astype(jnp.float32) for k in range(RING)]
    top = functools.reduce(jnp.maximum, stats)
    scales = [jnp.exp(x - top) for x in stats]
    total = functools.reduce(
        jnp.add,
        [
            scale * (pltpu.roll(x, LANES - 8, 1) + pltpu.roll(x, LANES - 16, 1))
            for scale, x in zip(scales, stats)
        ],
    )
    low = lanes_of((8, LANES)) < HALF
    mixed = []
    for b in range(blocks):
        acc = jnp.zeros((8, LANES), jnp.float32)
        for k in range(RING):
            acc = acc + parts[k, 8 * b : 8 * b + 8, :].astype(jnp.float32) * spread(
                scales[k], b, low
            )
        mixed.append(acc)
    return top, total, mixed, low


def combine(parts, out):
    top, total, mixed, _ = merged(parts)
    kind = lanes_of((8, LANES)) % 32
    total_high = rounded(total)
    stats = jnp.where(
        kind < 8,
        top,
        jnp.where(
            kind < 16, pltpu.roll(total_high, 8, 1), pltpu.roll(total - total_high, 16, 1)
        ),
    )
    line = jnp.concatenate([x.astype(jnp.bfloat16) for x in mixed + [stats]], axis=0)
    for k in range(RING):
        out[k] = line


def finish(parts, tokens, out_w, out, turned):
    _, total, mixed, low = merged(parts)
    inverse = 1.0 / total
    for b, acc in enumerate(mixed):
        turned[8 * b : 8 * b + 8, :] = rounded(acc * spread(inverse, b, low))
    count = tokens.shape[0]
    pairs = turned.shape[0] // count
    attended = jnp.concatenate(
        [turned[pl.ds(j, count, stride=pairs), :] for j in range(pairs)], axis=1
    ).astype(jnp.bfloat16)
    part = dotted(attended, out_w[...], 1)
    part = part + jnp.where(lax.axis_index("tp") == 0, tokens[...].astype(jnp.float32), 0.0)
    third = count // 2
    piece = jnp.concatenate((part[:third], part[third:]), axis=1).astype(jnp.bfloat16)
    for k in range(out.shape[0]):
        out[k] = piece


def mix(parts, gain, up_w, down_w, mid_out, out, mid):
    count, width = mid.shape
    third = count // 2
    low = lanes_of((third, LANES)) < HALF
    square = jnp.zeros((count, LANES), jnp.float32)
    for t in range(width // LANES):
        a = rounded(
            parts[4 * t].astype(jnp.float32) + parts[4 * t + 1].astype(jnp.float32)
        )
        b = rounded(
            parts[4 * t + 2].astype(jnp.float32) + parts[4 * t + 3].astype(jnp.float32)
        )
        at = slice(LANES * t, LANES * (t + 1))
        mid[:third, at] = jnp.where(low, a, pltpu.roll(b, HALF, 1))
        mid[third:, at] = jnp.where(low, pltpu.roll(a, HALF, 1), b)
        tile = mid[:, at]
        square = square + tile * tile
    scale = lax.rsqrt(jnp.sum(square, axis=1, keepdims=True) / D + epsilon)
    rows = mid[...]
    mid_out[...] = rows.astype(jnp.bfloat16)
    normed = (rows * gain[...] * scale).astype(jnp.bfloat16)
    hidden = jnp.square(jnp.maximum(dotted(normed, up_w[...]), 0.0))
    hidden = jnp.concatenate((hidden, jnp.zeros((8 - count, LANES), jnp.float32)), axis=0)
    picked = jnp.concatenate(
        [
            hidden[4 * a + (u + k) % 4 : 4 * a + (u + k) % 4 + 1]
            for k in range(4)
            for u in range(4)
            for a in range(2)
        ],
        axis=0,
    ).astype(jnp.bfloat16)
    spread_out = dotted(picked, down_w[...])
    group = lanes_of((8, LANES)) // 32
    owner = lax.broadcasted_iota(jnp.int32, (8, LANES), 0) // 2
    turn = (group - owner) % 4
    for t in range(width // LANES):
        at = slice(LANES * t, LANES * (t + 1))
        tile = spread_out[:8, at]
        for k in range(1, 4):
            tile = jnp.where(
                turn == k, pltpu.roll(spread_out[8 * k : 8 * k + 8, at], 32 * k, 1), tile
            )
        out[8 * t : 8 * t + 8, :] = tile.astype(jnp.bfloat16)


def close(parts, mid, out):
    total = jnp.zeros((8, LANES), jnp.float32)
    for t in range(parts.shape[0] // 8):
        total = total + parts[8 * t : 8 * t + 8, :].astype(jnp.float32)
    pair = total[0:2] + total[2:4] + total[4:6] + total[6:8]
    count, width = out.shape
    number = kv_spot() * 2 + lax.axis_index("tp")
    tile = mid[:, pl.ds(pl.multiple_of((number // 4) * LANES, LANES), LANES)]
    group = number % 4
    own = jnp.zeros((count, width), jnp.float32)
    for n in range(4):
        own = jnp.where(
            group == n, tile[:, width * n : width * (n + 1)].astype(jnp.float32), own
        )
    rows = [pair[r // 4 : r // 4 + 1, 32 * (r % 4) : 32 * (r % 4) + 32] for r in range(count)]
    out[...] = (own + jnp.concatenate(rows, axis=0)).astype(jnp.bfloat16)


def shards(
    tokens,
    lengths,
    attn_gain,
    query_weight,
    key_weight,
    value_weight,
    forget_weight,
    forget_offset,
    cache_keys,
    cache_values,
    gate_sum,
    out_weight,
    mlp_gain,
    up_weight,
    down_weight,
):
    rows, cols = tokens.shape
    bf16 = functools.partial(jax.ShapeDtypeStruct, dtype=jnp.bfloat16)
    stack = rows * query_weight.shape[1] // LANES
    line = stack + 16
    far = (tokens, attn_gain[None, :], query_weight, key_weight, value_weight, forget_weight.T)
    near = [pltpu.VMEM(x.shape, x.dtype) for x in far[:5]]
    x = call(
        project,
        bf16((RING, line, LANES)),
        [HBM] * 6,
        near
        + [
            pltpu.VMEM((forget_weight.shape[1], LANES), jnp.bfloat16),
            pltpu.VMEM((line, LANES), jnp.float32),
            pltpu.SemaphoreType.DMA((6,)),
        ],
    )(*[pltpu.with_memory_space_constraint(x, pltpu.HBM) for x in far])
    x = exchanged(x, "kv_1")
    x = call(resend, bf16((RING, line, LANES)), [VMEM])(x)
    x = exchanged(x, "kv_0")
    packed = stack + 8
    x = call(attend, bf16((RING, packed, LANES)), [VMEM] * 6)(
        lengths[None, :], forget_offset[None, :], x, cache_keys, cache_values, gate_sum
    )
    x = exchanged(x, "kv_1")
    x = call(combine, bf16((RING, packed, LANES)), [VMEM])(x)
    x = exchanged(x, "kv_0")
    group = lax.axis_size(KV_TP)
    x = call(
        finish,
        bf16((group, rows // 2, LANES)),
        [VMEM] * 3,
        [pltpu.VMEM((stack, LANES), jnp.float32)],
    )(x, tokens, out_weight.T)
    x = exchanged(x, KV_TP)
    mid, x = call(
        mix,
        (bf16((rows, D)), bf16((2 * group, LANES))),
        [VMEM] * 4,
        [pltpu.VMEM((rows, D), jnp.float32)],
    )(x, mlp_gain[None, :], up_weight, down_weight)
    x = exchanged(x.reshape(group, 2, LANES), KV_TP).reshape(2 * group, LANES)
    return call(close, bf16((rows, D // group)), [VMEM, VMEM])(x, mid)


def solution(mesh):
    torus = Mesh(
        mesh.devices.reshape(mesh.shape["dp"], 8, 8, mesh.shape["tp"]), ("dp", "kv_0", "kv_1", "tp")
    )
    placed = (
        P("dp", KV),
        P("dp"),
        P(KV),
        P(KV, "tp"),
        P(KV, "tp"),
        P(KV, "tp"),
        P(),
        P("tp"),
        P("dp", KV, "tp"),
        P("dp", KV, "tp"),
        P("dp", "tp", KV),
        P("tp", KV),
        P(),
        P(None, KV_TP),
        P(KV_TP, None),
    )
    return jax.shard_map(
        shards, mesh=torus, in_specs=placed, out_specs=P("dp", KV_TP), check_vma=False
    )
```

```python
import functools

import jax
import jax.numpy as jnp
from jax import lax
from jax.experimental import pallas as pl
from jax.experimental.pallas import tpu as pltpu
from jax.sharding import Mesh
from jax.sharding import PartitionSpec as P

D = 4096
HEADS = 64
HD = 64
KEY_VALUE_HEADS = 4
KV = ("kv_0", "kv_1")
KV_TP = ("kv_0", "kv_1", "tp")
LANES = 128
HALF = 64
RING = 8

epsilon = 1e-06
floor_score = -1e30

VMEM = pl.BlockSpec(memory_space=pltpu.VMEM)
HBM = pl.BlockSpec(memory_space=pltpu.HBM)


def call(body, out_shape, in_specs, scratch=(), flops=1 << 20):
    return pl.pallas_call(
        body,
        out_shape=out_shape,
        in_specs=in_specs,
        out_specs=jax.tree.map(lambda _: VMEM, out_shape),
        scratch_shapes=scratch,
        compiler_params=pltpu.CompilerParams(vmem_limit_bytes=16 << 20),
        cost_estimate=pl.CostEstimate(flops=flops, bytes_accessed=1 << 20, transcendentals=0),
    )


def lanes_of(shape):
    return lax.broadcasted_iota(jnp.int32, shape, len(shape) - 1)


def rounded(x):
    return x.astype(jnp.bfloat16).astype(jnp.float32)


def exchanged(x, axes):
    return lax.all_to_all(x, axes, split_axis=0, concat_axis=0, tiled=True)


def dotted(a, b, b_dim=0):
    return lax.dot_general(
        a, b, (((1,), (b_dim,)), ((), ())), preferred_element_type=jnp.float32
    )


def kv_spot():
    return lax.axis_index("kv_0") * lax.axis_size("kv_1") + lax.axis_index("kv_1")


def project(
    tokens_far, gain_far, query_far, key_far, value_far, forget_far, lengths_far, offsets_far,
    out, lengths, offsets,
    tokens, gain, query_w, key_w, value_w, forget_w, dense, arrived,
):
    spot = kv_spot()
    window = pl.ds(pl.multiple_of((spot // 2) * LANES, LANES), LANES)
    copies = [
        pltpu.make_async_copy(far, near, arrived.at[n])
        for n, (far, near) in enumerate(
            (
                (query_far, query_w),
                (tokens_far, tokens),
                (gain_far, gain),
                (key_far, key_w),
                (value_far, value_w),
                (forget_far.at[:, window], forget_w),
                (lengths_far, lengths),
                (offsets_far, offsets),
            )
        )
    ]
    for copy in copies:
        copy.start()
    for copy in copies[1:3]:
        copy.wait()
    rows = tokens[...].astype(jnp.float32)
    count, cols = rows.shape
    scaled = (rows * gain[...]).astype(jnp.bfloat16)
    wide = scaled.astype(jnp.float32)
    square = jnp.sum(rows * rows, axis=1, keepdims=True)
    square_high = rounded(square)
    for copy in copies[3:]:
        copy.wait()
    gates = forget_w[...].astype(jnp.float32)
    gates = jnp.where(spot % 2 == 0, gates[:, :cols], gates[:, cols:])
    columns = [
        jnp.sum(wide * gates[n : n + 1, :], axis=1, keepdims=True) for n in range(gates.shape[0])
    ] + [square_high, square - square_high]
    lane = lanes_of((count, LANES))
    extra = jnp.zeros(lane.shape, jnp.float32)
    for n, column in enumerate(columns):
        extra = jnp.where((lane == n) | (lane == n + HALF), column, extra)
    third = count // 2
    extra = jnp.where(lane[:third] < HALF, extra[:third], extra[third:])
    copies[0].wait()
    query = dotted(scaled, query_w[...])
    pairs = query.shape[1] // LANES
    stack = pairs * count
    for j in range(pairs):
        dense[pl.ds(j, count, stride=pairs), :] = query[:, LANES * j : LANES * (j + 1)]
    dense[stack : stack + count, :] = dotted(scaled, key_w[...])
    dense[stack + count : stack + 2 * count, :] = dotted(scaled, value_w[...])
    dense[stack + 2 * count : stack + 2 * count + third, :] = extra
    spare = stack + 2 * count + third
    dense[spare:, :] = jnp.zeros((dense.shape[0] - spare, LANES), jnp.float32)
    line = dense[...].astype(jnp.bfloat16)
    for k in range(RING):
        out[k] = line


def summed(parts):
    total = parts[0].astype(jnp.float32)
    for k in range(1, RING):
        total = total + parts[k].astype(jnp.float32)
    return total


def resend(parts, out):
    line = summed(parts).astype(jnp.bfloat16)
    for k in range(RING):
        out[k] = line


def attend(lengths, offsets, parts, keys, values, gate, out):
    count, positions = keys.shape[0], keys.shape[1]
    spot = kv_spot()
    line = summed(parts)
    stack = line.shape[0] - 16
    pairs = stack // count
    tail = line[stack:]
    third = count // 2
    extra = tail[2 * count : 2 * count + third]
    extra = jnp.concatenate((extra, extra), axis=0)
    lane = lanes_of((count, LANES))
    lane = lane - HALF * (lax.broadcasted_iota(jnp.int32, lane.shape, 0) // third)

    def picked(first, last):
        held = jnp.where((lane >= first) & (lane <= last), extra, 0.0)
        return jnp.broadcast_to(jnp.sum(held, axis=1, keepdims=True), lane.shape)

    row_scale = lax.rsqrt(picked(4, 5) / D + epsilon)
    head = 2 * lax.axis_index("tp")
    forget = []
    for n in range(2):
        z = picked(head + n, head + n) * row_scale + offsets[:, n : n + 1]
        forget.append(jnp.minimum(z, 0.0) - jnp.log1p(jnp.exp(-jnp.abs(z))))
    new_key = rounded(tail[:count] * row_scale)
    new_value = rounded(tail[count : 2 * count] * row_scale)
    every = range(count)
    lane = lanes_of((pairs, LANES))
    row = lax.broadcasted_iota(jnp.int32, (pairs, LANES), 0)
    straight = (lane < HALF) == (row < pairs // 2)
    first = spot == 0
    place_of = spot * positions + lanes_of((1, positions))
    live = [place_of < lengths[:, s : s + 1] for s in every]
    both = [rounded(line[pairs * s : pairs * (s + 1)] * row_scale[s : s + 1, :]) for s in every]
    rolled = [pltpu.roll(x, HALF, 1) for x in both]
    queries = [
        jnp.concatenate((jnp.where(straight, x, 0.0), jnp.where(straight, y, 0.0)), axis=0)
        for x, y in zip(both, rolled)
    ]
    scores = [dotted(queries[s].astype(jnp.bfloat16), keys[s], 1) * HD ** (-0.5) for s in every]
    owns = [
        jnp.sum(queries[s] * new_key[s : s + 1, :], axis=1, keepdims=True) * HD ** (-0.5)
        for s in every
    ]
    owns = [jnp.where(first, x, floor_score) for x in owns]
    for s in every:
        lines = [
            jnp.broadcast_to(
                gate[s, n : n + 1, :]
                + jnp.concatenate([forget[n][s : s + 1, :]] * (positions // LANES), axis=1),
                (8, positions),
            )
            for n in range(2)
        ]
        scores[s] = jnp.where(
            live[s], scores[s] + jnp.concatenate(lines + lines, axis=0), floor_score
        )
    tops = [
        rounded(jnp.maximum(jnp.max(scores[s], axis=1, keepdims=True), owns[s])) for s in every
    ]
    weights = [jnp.where(live[s], jnp.exp(scores[s] - tops[s]), 0.0) for s in every]
    own_weights = [jnp.where(first, jnp.exp(owns[s] - tops[s]), 0.0) for s in every]
    mixed = [dotted(weights[s].astype(jnp.bfloat16), values[s]) for s in every]
    totals = [jnp.sum(weights[s], axis=1, keepdims=True) + own_weights[s] for s in every]
    mixed = [mixed[s] + rounded(own_weights[s]) * new_value[s : s + 1, :] for s in every]
    rolled = [pltpu.roll(x[pairs:], HALF, 1) for x in mixed]
    blocks = [
        jnp.where(straight, mixed[s][:pairs], rolled[s]).astype(jnp.bfloat16) for s in every
    ]
    stat_lane = lanes_of((8, LANES))
    stats = jnp.zeros((8, LANES), jnp.float32)
    for s in every:
        total_high = rounded(totals[s])
        for n, column in enumerate((tops[s], total_high, totals[s] - total_high)):
            for g in range(4):
                stats = jnp.where(
                    stat_lane == 32 * g + 8 * n + s, column[8 * g : 8 * g + 8], stats
                )
    blocks.append(stats.astype(jnp.bfloat16))
    line = jnp.concatenate(blocks, axis=0)
    for k in range(RING):
        out[k] = line


def spread(compact, block):
    s, half = divmod(block, 2)
    left, right = (s, 64 + s) if half == 0 else (96 + s, 32 + s)
    source = jnp.where(lanes_of(compact.shape) < HALF, left, right)
    return jnp.take_along_axis(compact, source, axis=1, mode="promise_in_bounds")


def merged(parts):
    rows = parts.shape[1]
    blocks = rows // 8 - 1
    stats = [parts[k, rows - 8 : rows, :].astype(jnp.float32) for k in range(RING)]
    top = functools.reduce(jnp.maximum, stats)
    scales = [jnp.exp(x - top) for x in stats]
    total = functools.reduce(
        jnp.add,
        [
            scale * (pltpu.roll(x, LANES - 8, 1) + pltpu.roll(x, LANES - 16, 1))
            for scale, x in zip(scales, stats)
        ],
    )
    mixed = []
    for b in range(blocks):
        acc = jnp.zeros((8, LANES), jnp.float32)
        for k in range(RING):
            acc = acc + parts[k, 8 * b : 8 * b + 8, :].astype(jnp.float32) * spread(
                scales[k], b
            )
        mixed.append(acc)
    return top, total, mixed


def combine(parts, out):
    top, total, mixed = merged(parts)
    kind = lanes_of((8, LANES)) % 32
    total_high = rounded(total)
    stats = jnp.where(
        kind < 8,
        top,
        jnp.where(
            kind < 16, pltpu.roll(total_high, 8, 1), pltpu.roll(total - total_high, 16, 1)
        ),
    )
    line = jnp.concatenate([x.astype(jnp.bfloat16) for x in mixed + [stats]], axis=0)
    for k in range(RING):
        out[k] = line


def finish(parts, tokens, out_w, out, turned):
    _, total, mixed = merged(parts)
    inverse = 1.0 / total
    for b, acc in enumerate(mixed):
        turned[8 * b : 8 * b + 8, :] = rounded(acc * spread(inverse, b))
    count = tokens.shape[0]
    pairs = turned.shape[0] // count
    attended = jnp.concatenate(
        [turned[pl.ds(j, count, stride=pairs), :] for j in range(pairs)], axis=1
    ).astype(jnp.bfloat16)
    part = dotted(attended, out_w[...], 1)
    part = part + jnp.where(lax.axis_index("tp") == 0, tokens[...].astype(jnp.float32), 0.0)
    third = count // 2
    piece = jnp.concatenate((part[:third], part[third:]), axis=1).astype(jnp.bfloat16)
    for k in range(out.shape[0]):
        out[k] = piece


def mix(parts, gain, up_w, down_w, mid_out, out, mid):
    count, width = mid.shape
    third = count // 2
    low = lanes_of((third, LANES)) < HALF
    square = jnp.zeros((count, LANES), jnp.float32)
    for t in range(width // LANES):
        a = rounded(
            parts[4 * t].astype(jnp.float32) + parts[4 * t + 1].astype(jnp.float32)
        )
        b = rounded(
            parts[4 * t + 2].astype(jnp.float32) + parts[4 * t + 3].astype(jnp.float32)
        )
        at = slice(LANES * t, LANES * (t + 1))
        mid[:third, at] = jnp.where(low, a, pltpu.roll(b, HALF, 1))
        mid[third:, at] = jnp.where(low, pltpu.roll(a, HALF, 1), b)
        tile = mid[:, at]
        square = square + tile * tile
    scale = lax.rsqrt(jnp.sum(square, axis=1, keepdims=True) / D + epsilon)
    rows = mid[...]
    mid_out[...] = rows.astype(jnp.bfloat16)
    gained = (rows * gain[...]).astype(jnp.bfloat16)
    hidden = jnp.square(jnp.maximum(dotted(gained, up_w[...]) * scale, 0.0))
    hidden = jnp.concatenate((hidden, jnp.zeros((8 - count, LANES), jnp.float32)), axis=0)
    picked = jnp.concatenate(
        [
            hidden[4 * a + (u + k) % 4 : 4 * a + (u + k) % 4 + 1]
            for k in range(4)
            for u in range(4)
            for a in range(2)
        ],
        axis=0,
    ).astype(jnp.bfloat16)
    spread_out = dotted(picked, down_w[...])
    group = lanes_of((8, LANES)) // 32
    owner = lax.broadcasted_iota(jnp.int32, (8, LANES), 0) // 2
    turn = (group - owner) % 4
    for t in range(width // LANES):
        at = slice(LANES * t, LANES * (t + 1))
        tile = spread_out[:8, at]
        for k in range(1, 4):
            tile = jnp.where(
                turn == k, pltpu.roll(spread_out[8 * k : 8 * k + 8, at], 32 * k, 1), tile
            )
        out[8 * t : 8 * t + 8, :] = tile.astype(jnp.bfloat16)


def close(parts, mid, out):
    total = jnp.zeros((8, LANES), jnp.float32)
    for t in range(parts.shape[0] // 8):
        total = total + parts[8 * t : 8 * t + 8, :].astype(jnp.float32)
    pair = total[0:2] + total[2:4] + total[4:6] + total[6:8]
    count, width = out.shape
    number = kv_spot() * 2 + lax.axis_index("tp")
    tile = mid[:, pl.ds(pl.multiple_of((number // 4) * LANES, LANES), LANES)]
    turn = lax.rem(4 - number % 4, 4) * 32
    own = pltpu.roll(tile.astype(jnp.float32), turn, 1)
    turned = [pair if n == 0 else pltpu.roll(pair, LANES - 32 * n, 1) for n in range(4)]
    rows = [turned[r % 4][r // 4 : r // 4 + 1] for r in range(count)]
    out[...] = (own + jnp.concatenate(rows, axis=0))[:, :width].astype(jnp.bfloat16)


def shards(
    tokens,
    lengths,
    attn_gain,
    query_weight,
    key_weight,
    value_weight,
    forget_weight,
    forget_offset,
    cache_keys,
    cache_values,
    gate_sum,
    out_weight,
    mlp_gain,
    up_weight,
    down_weight,
):
    rows, cols = tokens.shape
    bf16 = functools.partial(jax.ShapeDtypeStruct, dtype=jnp.bfloat16)
    stack = rows * query_weight.shape[1] // LANES
    line = stack + 16
    far = (
        tokens,
        attn_gain[None, :],
        query_weight,
        key_weight,
        value_weight,
        forget_weight.T,
        lengths[None, :],
        forget_offset[None, :],
    )
    near = [pltpu.VMEM(x.shape, x.dtype) for x in far[:5]]
    x, lengths, forget_offset = call(
        project,
        (
            bf16((RING, line, LANES)),
            jax.ShapeDtypeStruct(far[6].shape, far[6].dtype),
            jax.ShapeDtypeStruct(far[7].shape, far[7].dtype),
        ),
        [HBM] * 8,
        near
        + [
            pltpu.VMEM((forget_weight.shape[1], LANES), jnp.bfloat16),
            pltpu.VMEM((line, LANES), jnp.float32),
            pltpu.SemaphoreType.DMA((8,)),
        ],
    )(*[pltpu.with_memory_space_constraint(x, pltpu.HBM) for x in far])
    x = exchanged(x, "kv_1")
    x = call(resend, bf16((RING, line, LANES)), [VMEM])(x)
    x = exchanged(x, "kv_0")
    packed = stack + 8
    x = call(attend, bf16((RING, packed, LANES)), [VMEM] * 6)(
        lengths, forget_offset, x, cache_keys, cache_values, gate_sum
    )
    x = exchanged(x, "kv_1")
    x = call(combine, bf16((RING, packed, LANES)), [VMEM])(x)
    x = exchanged(x, "kv_0")
    group = lax.axis_size(KV_TP)
    x = call(
        finish,
        bf16((group, rows // 2, LANES)),
        [VMEM] * 3,
        [pltpu.VMEM((stack, LANES), jnp.float32)],
    )(x, tokens, out_weight.T)
    x = exchanged(x, KV_TP)
    mid, x = call(
        mix,
        (bf16((rows, D)), bf16((2 * group, LANES))),
        [VMEM] * 4,
        [pltpu.VMEM((rows, D), jnp.float32)],
    )(x, mlp_gain[None, :], up_weight, down_weight)
    x = exchanged(x.reshape(group, 2, LANES), KV_TP).reshape(2 * group, LANES)
    return call(close, bf16((rows, D // group)), [VMEM, VMEM])(x, mid)


def solution(mesh):
    torus = Mesh(
        mesh.devices.reshape(mesh.shape["dp"], 8, 8, mesh.shape["tp"]), ("dp", "kv_0", "kv_1", "tp")
    )
    placed = (
        P("dp", KV),
        P("dp"),
        P(KV),
        P(KV, "tp"),
        P(KV, "tp"),
        P(KV, "tp"),
        P(),
        P("tp"),
        P("dp", KV, "tp"),
        P("dp", KV, "tp"),
        P("dp", "tp", KV),
        P("tp", KV),
        P(),
        P(None, KV_TP),
        P(KV_TP, None),
    )
    return jax.shard_map(
        shards, mesh=torus, in_specs=placed, out_specs=P("dp", KV_TP), check_vma=False
    )
```

```python
import functools

import jax
import jax.numpy as jnp
from jax import lax
from jax.experimental import pallas as pl
from jax.experimental.pallas import tpu as pltpu
from jax.sharding import Mesh
from jax.sharding import PartitionSpec as P

D = 4096
HEADS = 64
HD = 64
KEY_VALUE_HEADS = 4
KV = ("kv_0", "kv_1")
KV_TP = ("kv_0", "kv_1", "tp")
LANES = 128
HALF = 64
RING = 8
RING_ORDER = (0, 4, 2, 6, 3, 7, 1, 5)

epsilon = 1e-06
floor_score = -1e30

VMEM = pl.BlockSpec(memory_space=pltpu.VMEM)
HBM = pl.BlockSpec(memory_space=pltpu.HBM)


def call(body, out_shape, in_specs, scratch=(), flops=1 << 20):
    return pl.pallas_call(
        body,
        out_shape=out_shape,
        in_specs=in_specs,
        out_specs=jax.tree.map(lambda _: VMEM, out_shape),
        scratch_shapes=scratch,
        compiler_params=pltpu.CompilerParams(vmem_limit_bytes=16 << 20),
        cost_estimate=pl.CostEstimate(flops=flops, bytes_accessed=1 << 20, transcendentals=0),
    )


def lanes_of(shape):
    return lax.broadcasted_iota(jnp.int32, shape, len(shape) - 1)


def rounded(x):
    return x.astype(jnp.bfloat16).astype(jnp.float32)


def exchanged(x, groups):
    return lax.all_to_all(
        x, KV_TP, split_axis=0, concat_axis=0, axis_index_groups=groups, tiled=True
    )


def ring_groups(along_last):
    def member(fixed, moving, core):
        first, last = (fixed, moving) if along_last else (moving, fixed)
        return (first * RING + last) * 2 + core

    return [
        [member(fixed, moving, core) for moving in RING_ORDER]
        for core in range(2)
        for fixed in range(RING)
    ]


def dotted(a, b, b_dim=0):
    return lax.dot_general(
        a, b, (((1,), (b_dim,)), ((), ())), preferred_element_type=jnp.float32
    )


def kv_spot():
    return lax.axis_index("kv_0") * lax.axis_size("kv_1") + lax.axis_index("kv_1")


def project(
    tokens_far, gain_far, query_far, key_far, value_far, forget_far, lengths_far, offsets_far,
    out, lengths, offsets,
    tokens, gain, query_w, key_w, value_w, forget_w, dense, arrived,
):
    spot = kv_spot()
    window = pl.ds(pl.multiple_of((spot // 2) * LANES, LANES), LANES)
    copies = [
        pltpu.make_async_copy(far, near, arrived.at[n])
        for n, (far, near) in enumerate(
            (
                (query_far, query_w),
                (tokens_far, tokens),
                (gain_far, gain),
                (key_far, key_w),
                (value_far, value_w),
                (forget_far.at[:, window], forget_w),
                (lengths_far, lengths),
                (offsets_far, offsets),
            )
        )
    ]
    for copy in copies:
        copy.start()
    for copy in copies[1:3]:
        copy.wait()
    rows = tokens[...].astype(jnp.float32)
    count, cols = rows.shape
    scaled = (rows * gain[...]).astype(jnp.bfloat16)
    wide = scaled.astype(jnp.float32)
    square = jnp.sum(rows * rows, axis=1, keepdims=True)
    square_high = rounded(square)
    for copy in copies[3:]:
        copy.wait()
    gates = forget_w[...].astype(jnp.float32)
    gates = jnp.where(spot % 2 == 0, gates[:, :cols], gates[:, cols:])
    columns = [
        jnp.sum(wide * gates[n : n + 1, :], axis=1, keepdims=True) for n in range(gates.shape[0])
    ] + [square_high, square - square_high]
    lane = lanes_of((count, LANES))
    extra = jnp.zeros(lane.shape, jnp.float32)
    for n, column in enumerate(columns):
        extra = jnp.where((lane == n) | (lane == n + HALF), column, extra)
    third = count // 2
    extra = jnp.where(lane[:third] < HALF, extra[:third], extra[third:])
    copies[0].wait()
    query = dotted(scaled, query_w[...])
    pairs = query.shape[1] // LANES
    stack = pairs * count
    for j in range(pairs):
        dense[pl.ds(j, count, stride=pairs), :] = query[:, LANES * j : LANES * (j + 1)]
    dense[stack : stack + count, :] = dotted(scaled, key_w[...])
    dense[stack + count : stack + 2 * count, :] = dotted(scaled, value_w[...])
    dense[stack + 2 * count : stack + 2 * count + third, :] = extra
    spare = stack + 2 * count + third
    dense[spare:, :] = jnp.zeros((dense.shape[0] - spare, LANES), jnp.float32)
    line = dense[...].astype(jnp.bfloat16)
    for k in range(RING):
        out[k] = line


def summed(parts):
    total = parts[0].astype(jnp.float32)
    for k in range(1, RING):
        total = total + parts[k].astype(jnp.float32)
    return total


def resend(parts, out):
    line = summed(parts).astype(jnp.bfloat16)
    for k in range(RING):
        out[k] = line


def attend(lengths, offsets, parts, keys, values, gate, out):
    count, positions = keys.shape[0], keys.shape[1]
    spot = kv_spot()
    line = summed(parts)
    stack = line.shape[0] - 16
    pairs = stack // count
    tail = line[stack:]
    third = count // 2
    extra = tail[2 * count : 2 * count + third]
    extra = jnp.concatenate((extra, extra), axis=0)
    lane = lanes_of((count, LANES))
    lane = lane - HALF * (lax.broadcasted_iota(jnp.int32, lane.shape, 0) // third)

    def picked(first, last):
        held = jnp.where((lane >= first) & (lane <= last), extra, 0.0)
        return jnp.broadcast_to(jnp.sum(held, axis=1, keepdims=True), lane.shape)

    row_scale = lax.rsqrt(picked(4, 5) / D + epsilon)
    head = 2 * lax.axis_index("tp")
    forget = []
    for n in range(2):
        z = picked(head + n, head + n) * row_scale + offsets[:, n : n + 1]
        forget.append(jnp.minimum(z, 0.0) - jnp.log1p(jnp.exp(-jnp.abs(z))))
    new_key = rounded(tail[:count] * row_scale)
    new_value = rounded(tail[count : 2 * count] * row_scale)
    every = range(count)
    lane = lanes_of((pairs, LANES))
    row = lax.broadcasted_iota(jnp.int32, (pairs, LANES), 0)
    straight = (lane < HALF) == (row < pairs // 2)
    first = spot == 0
    place_of = spot * positions + lanes_of((1, positions))
    live = [place_of < lengths[:, s : s + 1] for s in every]
    both = [rounded(line[pairs * s : pairs * (s + 1)] * row_scale[s : s + 1, :]) for s in every]
    rolled = [pltpu.roll(x, HALF, 1) for x in both]
    queries = [
        jnp.concatenate((jnp.where(straight, x, 0.0), jnp.where(straight, y, 0.0)), axis=0)
        for x, y in zip(both, rolled)
    ]
    scores = [dotted(queries[s].astype(jnp.bfloat16), keys[s], 1) * HD ** (-0.5) for s in every]
    owns = [
        jnp.sum(queries[s] * new_key[s : s + 1, :], axis=1, keepdims=True) * HD ** (-0.5)
        for s in every
    ]
    owns = [jnp.where(first, x, floor_score) for x in owns]
    for s in every:
        lines = [
            jnp.broadcast_to(
                gate[s, n : n + 1, :]
                + jnp.concatenate([forget[n][s : s + 1, :]] * (positions // LANES), axis=1),
                (8, positions),
            )
            for n in range(2)
        ]
        scores[s] = jnp.where(
            live[s], scores[s] + jnp.concatenate(lines + lines, axis=0), floor_score
        )
    tops = [
        rounded(jnp.maximum(jnp.max(scores[s], axis=1, keepdims=True), owns[s])) for s in every
    ]
    weights = [jnp.where(live[s], jnp.exp(scores[s] - tops[s]), 0.0) for s in every]
    own_weights = [jnp.where(first, jnp.exp(owns[s] - tops[s]), 0.0) for s in every]
    mixed = [dotted(weights[s].astype(jnp.bfloat16), values[s]) for s in every]
    totals = [jnp.sum(weights[s], axis=1, keepdims=True) + own_weights[s] for s in every]
    mixed = [mixed[s] + rounded(own_weights[s]) * new_value[s : s + 1, :] for s in every]
    rolled = [pltpu.roll(x[pairs:], HALF, 1) for x in mixed]
    blocks = [
        jnp.where(straight, mixed[s][:pairs], rolled[s]).astype(jnp.bfloat16) for s in every
    ]
    stat_lane = lanes_of((8, LANES))
    stats = jnp.zeros((8, LANES), jnp.float32)
    for s in every:
        total_high = rounded(totals[s])
        for n, column in enumerate((tops[s], total_high, totals[s] - total_high)):
            for g in range(4):
                stats = jnp.where(
                    stat_lane == 32 * g + 8 * n + s, column[8 * g : 8 * g + 8], stats
                )
    blocks.append(stats.astype(jnp.bfloat16))
    line = jnp.concatenate(blocks, axis=0)
    for k in range(RING):
        out[k] = line


def spread(compact, block):
    s, half = divmod(block, 2)
    left, right = (s, 64 + s) if half == 0 else (96 + s, 32 + s)
    source = jnp.where(lanes_of(compact.shape) < HALF, left, right)
    return jnp.take_along_axis(compact, source, axis=1, mode="promise_in_bounds")


def merged(parts):
    rows = parts.shape[1]
    blocks = rows // 8 - 1
    stats = [parts[k, rows - 8 : rows, :].astype(jnp.float32) for k in range(RING)]
    top = functools.reduce(jnp.maximum, stats)
    scales = [jnp.exp(x - top) for x in stats]
    total = functools.reduce(
        jnp.add,
        [
            scale * (pltpu.roll(x, LANES - 8, 1) + pltpu.roll(x, LANES - 16, 1))
            for scale, x in zip(scales, stats)
        ],
    )
    mixed = []
    for b in range(blocks):
        acc = jnp.zeros((8, LANES), jnp.float32)
        for k in range(RING):
            acc = acc + parts[k, 8 * b : 8 * b + 8, :].astype(jnp.float32) * spread(
                scales[k], b
            )
        mixed.append(acc)
    return top, total, mixed


def combine(parts, out):
    top, total, mixed = merged(parts)
    kind = lanes_of((8, LANES)) % 32
    total_high = rounded(total)
    stats = jnp.where(
        kind < 8,
        top,
        jnp.where(
            kind < 16, pltpu.roll(total_high, 8, 1), pltpu.roll(total - total_high, 16, 1)
        ),
    )
    line = jnp.concatenate([x.astype(jnp.bfloat16) for x in mixed + [stats]], axis=0)
    for k in range(RING):
        out[k] = line


def finish(parts, tokens, out_w, out, turned):
    _, total, mixed = merged(parts)
    inverse = 1.0 / total
    for b, acc in enumerate(mixed):
        turned[8 * b : 8 * b + 8, :] = rounded(acc * spread(inverse, b))
    count = tokens.shape[0]
    pairs = turned.shape[0] // count
    attended = jnp.concatenate(
        [turned[pl.ds(j, count, stride=pairs), :] for j in range(pairs)], axis=1
    ).astype(jnp.bfloat16)
    part = dotted(attended, out_w[...], 1)
    part = part + jnp.where(lax.axis_index("tp") == 0, tokens[...].astype(jnp.float32), 0.0)
    third = count // 2
    piece = jnp.concatenate((part[:third], part[third:]), axis=1).astype(jnp.bfloat16)
    for k in range(out.shape[0]):
        out[k] = piece


def mix(parts, gain, up_w, down_w, mid_out, out, mid):
    count, width = mid.shape
    third = count // 2
    low = lanes_of((third, LANES)) < HALF
    square = jnp.zeros((count, LANES), jnp.float32)
    for t in range(width // LANES):
        a = rounded(
            parts[4 * t].astype(jnp.float32) + parts[4 * t + 1].astype(jnp.float32)
        )
        b = rounded(
            parts[4 * t + 2].astype(jnp.float32) + parts[4 * t + 3].astype(jnp.float32)
        )
        at = slice(LANES * t, LANES * (t + 1))
        mid[:third, at] = jnp.where(low, a, pltpu.roll(b, HALF, 1))
        mid[third:, at] = jnp.where(low, pltpu.roll(a, HALF, 1), b)
        tile = mid[:, at]
        square = square + tile * tile
    scale = lax.rsqrt(jnp.sum(square, axis=1, keepdims=True) / D + epsilon)
    rows = mid[...]
    mid_out[...] = rows.astype(jnp.bfloat16)
    gained = (rows * gain[...]).astype(jnp.bfloat16)
    hidden = jnp.square(jnp.maximum(dotted(gained, up_w[...]) * scale, 0.0))
    hidden = jnp.concatenate((hidden, jnp.zeros((8 - count, LANES), jnp.float32)), axis=0)
    picked = jnp.concatenate(
        [
            hidden[4 * a + (u + k) % 4 : 4 * a + (u + k) % 4 + 1]
            for k in range(4)
            for u in range(4)
            for a in range(2)
        ],
        axis=0,
    ).astype(jnp.bfloat16)
    spread_out = dotted(picked, down_w[...])
    group = lanes_of((8, LANES)) // 32
    owner = lax.broadcasted_iota(jnp.int32, (8, LANES), 0) // 2
    turn = (group - owner) % 4
    for t in range(width // LANES):
        at = slice(LANES * t, LANES * (t + 1))
        tile = spread_out[:8, at]
        for k in range(1, 4):
            tile = jnp.where(
                turn == k, pltpu.roll(spread_out[8 * k : 8 * k + 8, at], 32 * k, 1), tile
            )
        out[8 * t : 8 * t + 8, :] = tile.astype(jnp.bfloat16)


def close(parts, mid, out):
    total = jnp.zeros((8, LANES), jnp.float32)
    for t in range(parts.shape[0] // 8):
        total = total + parts[8 * t : 8 * t + 8, :].astype(jnp.float32)
    pair = total[0:2] + total[2:4] + total[4:6] + total[6:8]
    count, width = out.shape
    number = kv_spot() * 2 + lax.axis_index("tp")
    tile = mid[:, pl.ds(pl.multiple_of((number // 4) * LANES, LANES), LANES)]
    turn = lax.rem(4 - number % 4, 4) * 32
    own = pltpu.roll(tile.astype(jnp.float32), turn, 1)
    turned = [pair if n == 0 else pltpu.roll(pair, LANES - 32 * n, 1) for n in range(4)]
    rows = [turned[r % 4][r // 4 : r // 4 + 1] for r in range(count)]
    out[...] = (own + jnp.concatenate(rows, axis=0))[:, :width].astype(jnp.bfloat16)


def shards(
    tokens,
    lengths,
    attn_gain,
    query_weight,
    key_weight,
    value_weight,
    forget_weight,
    forget_offset,
    cache_keys,
    cache_values,
    gate_sum,
    out_weight,
    mlp_gain,
    up_weight,
    down_weight,
):
    rows, cols = tokens.shape
    bf16 = functools.partial(jax.ShapeDtypeStruct, dtype=jnp.bfloat16)
    stack = rows * query_weight.shape[1] // LANES
    line = stack + 16
    far = (
        tokens,
        attn_gain[None, :],
        query_weight,
        key_weight,
        value_weight,
        forget_weight.T,
        lengths[None, :],
        forget_offset[None, :],
    )
    near = [pltpu.VMEM(x.shape, x.dtype) for x in far[:5]]
    x, lengths, forget_offset = call(
        project,
        (
            bf16((RING, line, LANES)),
            jax.ShapeDtypeStruct(far[6].shape, far[6].dtype),
            jax.ShapeDtypeStruct(far[7].shape, far[7].dtype),
        ),
        [HBM] * 8,
        near
        + [
            pltpu.VMEM((forget_weight.shape[1], LANES), jnp.bfloat16),
            pltpu.VMEM((line, LANES), jnp.float32),
            pltpu.SemaphoreType.DMA((8,)),
        ],
    )(*[pltpu.with_memory_space_constraint(x, pltpu.HBM) for x in far])
    x = exchanged(x, ring_groups(True))
    x = call(resend, bf16((RING, line, LANES)), [VMEM])(x)
    x = exchanged(x, ring_groups(False))
    packed = stack + 8
    x = call(attend, bf16((RING, packed, LANES)), [VMEM] * 6)(
        lengths, forget_offset, x, cache_keys, cache_values, gate_sum
    )
    x = exchanged(x, ring_groups(True))
    x = call(combine, bf16((RING, packed, LANES)), [VMEM])(x)
    x = exchanged(x, ring_groups(False))
    group = lax.axis_size(KV_TP)
    x = call(
        finish,
        bf16((group, rows // 2, LANES)),
        [VMEM] * 3,
        [pltpu.VMEM((stack, LANES), jnp.float32)],
    )(x, tokens, out_weight.T)
    x = exchanged(x, None)
    mid, x = call(
        mix,
        (bf16((rows, D)), bf16((2 * group, LANES))),
        [VMEM] * 4,
        [pltpu.VMEM((rows, D), jnp.float32)],
    )(x, mlp_gain[None, :], up_weight, down_weight)
    x = exchanged(x.reshape(group, 2, LANES), None).reshape(2 * group, LANES)
    return call(close, bf16((rows, D // group)), [VMEM, VMEM])(x, mid)


def solution(mesh):
    torus = Mesh(
        mesh.devices.reshape(mesh.shape["dp"], 8, 8, mesh.shape["tp"]), ("dp", "kv_0", "kv_1", "tp")
    )
    placed = (
        P("dp", KV),
        P("dp"),
        P(KV),
        P(KV, "tp"),
        P(KV, "tp"),
        P(KV, "tp"),
        P(),
        P("tp"),
        P("dp", KV, "tp"),
        P("dp", KV, "tp"),
        P("dp", "tp", KV),
        P("tp", KV),
        P(),
        P(None, KV_TP),
        P(KV_TP, None),
    )
    return jax.shard_map(
        shards, mesh=torus, in_specs=placed, out_specs=P("dp", KV_TP), check_vma=False
    )
```

```python
import functools

import jax
import jax.numpy as jnp
from jax import lax
from jax.experimental import pallas as pl
from jax.experimental.pallas import tpu as pltpu
from jax.sharding import Mesh
from jax.sharding import PartitionSpec as P

D = 4096
HEADS = 64
HD = 64
KEY_VALUE_HEADS = 4
KV = ("kv_0", "kv_1")
KV_TP = ("kv_0", "kv_1", "tp")
LANES = 128
HALF = 64
RING = 8
RING_ORDER = (0, 2, 4, 6, 1, 3, 5, 7)

epsilon = 1e-06
floor_score = -1e30

VMEM = pl.BlockSpec(memory_space=pltpu.VMEM)
HBM = pl.BlockSpec(memory_space=pltpu.HBM)


def call(body, out_shape, in_specs, scratch=(), flops=1 << 20):
    return pl.pallas_call(
        body,
        out_shape=out_shape,
        in_specs=in_specs,
        out_specs=jax.tree.map(lambda _: VMEM, out_shape),
        scratch_shapes=scratch,
        compiler_params=pltpu.CompilerParams(vmem_limit_bytes=16 << 20),
        cost_estimate=pl.CostEstimate(flops=flops, bytes_accessed=1 << 20, transcendentals=0),
    )


def lanes_of(shape):
    return lax.broadcasted_iota(jnp.int32, shape, len(shape) - 1)


def rounded(x):
    return x.astype(jnp.bfloat16).astype(jnp.float32)


def exchanged(x, groups):
    return lax.all_to_all(
        x, KV_TP, split_axis=0, concat_axis=0, axis_index_groups=groups, tiled=True
    )


def ring_groups(along_last):
    def member(fixed, moving, core):
        first, last = (fixed, moving) if along_last else (moving, fixed)
        return (first * RING + last) * 2 + core

    return [
        [member(fixed, moving, core) for moving in RING_ORDER]
        for core in range(2)
        for fixed in range(RING)
    ]


def dotted(a, b, b_dim=0):
    return lax.dot_general(
        a, b, (((1,), (b_dim,)), ((), ())), preferred_element_type=jnp.float32
    )


def kv_spot():
    return lax.axis_index("kv_0") * lax.axis_size("kv_1") + lax.axis_index("kv_1")


def project(
    tokens_far, gain_far, query_far, key_far, value_far, forget_far, lengths_far, offsets_far,
    out, lengths, offsets,
    tokens, gain, query_w, key_w, value_w, forget_w, dense, arrived,
):
    spot = kv_spot()
    window = pl.ds(pl.multiple_of((spot // 2) * LANES, LANES), LANES)
    copies = [
        pltpu.make_async_copy(far, near, arrived.at[n])
        for n, (far, near) in enumerate(
            (
                (query_far, query_w),
                (tokens_far, tokens),
                (gain_far, gain),
                (key_far, key_w),
                (value_far, value_w),
                (forget_far.at[:, window], forget_w),
                (lengths_far, lengths),
                (offsets_far, offsets),
            )
        )
    ]
    for copy in copies:
        copy.start()
    for copy in copies[1:3]:
        copy.wait()
    rows = tokens[...].astype(jnp.float32)
    count, cols = rows.shape
    scaled = (rows * gain[...]).astype(jnp.bfloat16)
    wide = scaled.astype(jnp.float32)
    square = jnp.sum(rows * rows, axis=1, keepdims=True)
    square_high = rounded(square)
    for copy in copies[3:]:
        copy.wait()
    gates = forget_w[...].astype(jnp.float32)
    gates = jnp.where(spot % 2 == 0, gates[:, :cols], gates[:, cols:])
    columns = [
        jnp.sum(wide * gates[n : n + 1, :], axis=1, keepdims=True) for n in range(gates.shape[0])
    ] + [square_high, square - square_high]
    lane = lanes_of((count, LANES))
    extra = jnp.zeros(lane.shape, jnp.float32)
    for n, column in enumerate(columns):
        extra = jnp.where((lane == n) | (lane == n + HALF), column, extra)
    third = count // 2
    extra = jnp.where(lane[:third] < HALF, extra[:third], extra[third:])
    copies[0].wait()
    query = dotted(scaled, query_w[...])
    pairs = query.shape[1] // LANES
    stack = pairs * count
    for j in range(pairs):
        dense[pl.ds(j, count, stride=pairs), :] = query[:, LANES * j : LANES * (j + 1)]
    dense[stack : stack + count, :] = dotted(scaled, key_w[...])
    dense[stack + count : stack + 2 * count, :] = dotted(scaled, value_w[...])
    dense[stack + 2 * count : stack + 2 * count + third, :] = extra
    spare = stack + 2 * count + third
    dense[spare:, :] = jnp.zeros((dense.shape[0] - spare, LANES), jnp.float32)
    line = dense[...].astype(jnp.bfloat16)
    for k in range(RING):
        out[k] = line


def summed(parts):
    total = parts[0].astype(jnp.float32)
    for k in range(1, RING):
        total = total + parts[k].astype(jnp.float32)
    return total


def resend(parts, out):
    line = summed(parts).astype(jnp.bfloat16)
    for k in range(RING):
        out[k] = line


def attend(lengths, offsets, parts, keys, values, gate, out):
    count, positions = keys.shape[0], keys.shape[1]
    spot = kv_spot()
    line = summed(parts)
    stack = line.shape[0] - 16
    pairs = stack // count
    tail = line[stack:]
    third = count // 2
    extra = tail[2 * count : 2 * count + third]
    extra = jnp.concatenate((extra, extra), axis=0)
    lane = lanes_of((count, LANES))
    lane = lane - HALF * (lax.broadcasted_iota(jnp.int32, lane.shape, 0) // third)

    def picked(first, last):
        held = jnp.where((lane >= first) & (lane <= last), extra, 0.0)
        return jnp.broadcast_to(jnp.sum(held, axis=1, keepdims=True), lane.shape)

    row_scale = lax.rsqrt(picked(4, 5) / D + epsilon)
    head = 2 * lax.axis_index("tp")
    forget = []
    for n in range(2):
        z = picked(head + n, head + n) * row_scale + offsets[:, n : n + 1]
        forget.append(jnp.minimum(z, 0.0) - jnp.log1p(jnp.exp(-jnp.abs(z))))
    new_key = rounded(tail[:count] * row_scale)
    new_value = rounded(tail[count : 2 * count] * row_scale)
    every = range(count)
    lane = lanes_of((pairs, LANES))
    row = lax.broadcasted_iota(jnp.int32, (pairs, LANES), 0)
    straight = (lane < HALF) == (row < pairs // 2)
    first = spot == 0
    place_of = spot * positions + lanes_of((1, positions))
    live = [place_of < lengths[:, s : s + 1] for s in every]
    both = [rounded(line[pairs * s : pairs * (s + 1)] * row_scale[s : s + 1, :]) for s in every]
    rolled = [pltpu.roll(x, HALF, 1) for x in both]
    queries = [
        jnp.concatenate((jnp.where(straight, x, 0.0), jnp.where(straight, y, 0.0)), axis=0)
        for x, y in zip(both, rolled)
    ]
    scores = [dotted(queries[s].astype(jnp.bfloat16), keys[s], 1) * HD ** (-0.5) for s in every]
    owns = [
        jnp.sum(queries[s] * new_key[s : s + 1, :], axis=1, keepdims=True) * HD ** (-0.5)
        for s in every
    ]
    owns = [jnp.where(first, x, floor_score) for x in owns]
    for s in every:
        lines = [
            jnp.broadcast_to(
                gate[s, n : n + 1, :]
                + jnp.concatenate([forget[n][s : s + 1, :]] * (positions // LANES), axis=1),
                (8, positions),
            )
            for n in range(2)
        ]
        scores[s] = jnp.where(
            live[s], scores[s] + jnp.concatenate(lines + lines, axis=0), floor_score
        )
    tops = [
        rounded(jnp.maximum(jnp.max(scores[s], axis=1, keepdims=True), owns[s])) for s in every
    ]
    weights = [jnp.where(live[s], jnp.exp(scores[s] - tops[s]), 0.0) for s in every]
    own_weights = [jnp.where(first, jnp.exp(owns[s] - tops[s]), 0.0) for s in every]
    mixed = [dotted(weights[s].astype(jnp.bfloat16), values[s]) for s in every]
    totals = [jnp.sum(weights[s], axis=1, keepdims=True) + own_weights[s] for s in every]
    mixed = [mixed[s] + rounded(own_weights[s]) * new_value[s : s + 1, :] for s in every]
    rolled = [pltpu.roll(x[pairs:], HALF, 1) for x in mixed]
    blocks = [
        jnp.where(straight, mixed[s][:pairs], rolled[s]).astype(jnp.bfloat16) for s in every
    ]
    stat_lane = lanes_of((8, LANES))
    stats = jnp.zeros((8, LANES), jnp.float32)
    for s in every:
        total_high = rounded(totals[s])
        for n, column in enumerate((tops[s], total_high, totals[s] - total_high)):
            for g in range(4):
                stats = jnp.where(
                    stat_lane == 32 * g + 8 * n + s, column[8 * g : 8 * g + 8], stats
                )
    blocks.append(stats.astype(jnp.bfloat16))
    line = jnp.concatenate(blocks, axis=0)
    for k in range(RING):
        out[k] = line


def spread(compact, block):
    s, half = divmod(block, 2)
    left, right = (s, 64 + s) if half == 0 else (96 + s, 32 + s)
    source = jnp.where(lanes_of(compact.shape) < HALF, left, right)
    return jnp.take_along_axis(compact, source, axis=1, mode="promise_in_bounds")


def merged(parts):
    rows = parts.shape[1]
    blocks = rows // 8 - 1
    stats = [parts[k, rows - 8 : rows, :].astype(jnp.float32) for k in range(RING)]
    top = functools.reduce(jnp.maximum, stats)
    scales = [jnp.exp(x - top) for x in stats]
    total = functools.reduce(
        jnp.add,
        [
            scale * (pltpu.roll(x, LANES - 8, 1) + pltpu.roll(x, LANES - 16, 1))
            for scale, x in zip(scales, stats)
        ],
    )
    mixed = []
    for b in range(blocks):
        acc = jnp.zeros((8, LANES), jnp.float32)
        for k in range(RING):
            acc = acc + parts[k, 8 * b : 8 * b + 8, :].astype(jnp.float32) * spread(
                scales[k], b
            )
        mixed.append(acc)
    return top, total, mixed


def combine(parts, out):
    top, total, mixed = merged(parts)
    kind = lanes_of((8, LANES)) % 32
    total_high = rounded(total)
    stats = jnp.where(
        kind < 8,
        top,
        jnp.where(
            kind < 16, pltpu.roll(total_high, 8, 1), pltpu.roll(total - total_high, 16, 1)
        ),
    )
    line = jnp.concatenate([x.astype(jnp.bfloat16) for x in mixed + [stats]], axis=0)
    for k in range(RING):
        out[k] = line


def finish(parts, tokens, out_w, out, turned):
    _, total, mixed = merged(parts)
    inverse = 1.0 / total
    for b, acc in enumerate(mixed):
        turned[8 * b : 8 * b + 8, :] = rounded(acc * spread(inverse, b))
    count = tokens.shape[0]
    pairs = turned.shape[0] // count
    attended = jnp.concatenate(
        [turned[pl.ds(j, count, stride=pairs), :] for j in range(pairs)], axis=1
    ).astype(jnp.bfloat16)
    part = dotted(attended, out_w[...], 1)
    part = part + jnp.where(lax.axis_index("tp") == 0, tokens[...].astype(jnp.float32), 0.0)
    third = count // 2
    upper, lower = part[:third], part[third:]
    even = kv_spot() % 2 == 0
    piece = jnp.where(
        even,
        jnp.concatenate((upper, lower), axis=1),
        jnp.concatenate((lower, upper), axis=1),
    ).astype(jnp.bfloat16)
    for k in range(out.shape[0]):
        out[k] = piece


def mix(parts, gain, up_w, down_w, mid_out, out, mid):
    count, width = mid.shape
    third = count // 2
    low = lanes_of((third, LANES)) < HALF
    square = jnp.zeros((count, LANES), jnp.float32)
    for t in range(width // LANES):
        a = rounded(
            parts[4 * t].astype(jnp.float32) + parts[4 * t + 1].astype(jnp.float32)
        )
        b = rounded(
            parts[4 * t + 2].astype(jnp.float32) + parts[4 * t + 3].astype(jnp.float32)
        )
        at = slice(LANES * t, LANES * (t + 1))
        mid[:third, at] = jnp.where(low, a, b)
        mid[third:, at] = pltpu.roll(jnp.where(low, b, a), HALF, 1)
        tile = mid[:, at]
        square = square + tile * tile
    scale = lax.rsqrt(jnp.sum(square, axis=1, keepdims=True) / D + epsilon)
    rows = mid[...]
    mid_out[...] = rows.astype(jnp.bfloat16)
    gained = (rows * gain[...]).astype(jnp.bfloat16)
    hidden = jnp.square(jnp.maximum(dotted(gained, up_w[...]) * scale, 0.0))
    hidden = jnp.concatenate((hidden, jnp.zeros((8 - count, LANES), jnp.float32)), axis=0)
    picked = jnp.concatenate(
        [
            hidden[4 * a + (u + k) % 4 : 4 * a + (u + k) % 4 + 1]
            for k in range(4)
            for u in range(4)
            for a in range(2)
        ],
        axis=0,
    ).astype(jnp.bfloat16)
    spread_out = dotted(picked, down_w[...])
    group = lanes_of((8, LANES)) // 32
    owner = lax.broadcasted_iota(jnp.int32, (8, LANES), 0) // 2
    turn = (group - owner) % 4
    for t in range(width // LANES):
        at = slice(LANES * t, LANES * (t + 1))
        tile = spread_out[:8, at]
        for k in range(1, 4):
            tile = jnp.where(
                turn == k, pltpu.roll(spread_out[8 * k : 8 * k + 8, at], 32 * k, 1), tile
            )
        out[8 * t : 8 * t + 8, :] = tile.astype(jnp.bfloat16)


def close(parts, mid, out):
    total = jnp.zeros((8, LANES), jnp.float32)
    for t in range(parts.shape[0] // 8):
        total = total + parts[8 * t : 8 * t + 8, :].astype(jnp.float32)
    pair = total[0:2] + total[2:4] + total[4:6] + total[6:8]
    count, width = out.shape
    number = kv_spot() * 2 + lax.axis_index("tp")
    tile = mid[:, pl.ds(pl.multiple_of((number // 4) * LANES, LANES), LANES)]
    turn = lax.rem(4 - number % 4, 4) * 32
    own = pltpu.roll(tile.astype(jnp.float32), turn, 1)
    turned = [pair if n == 0 else pltpu.roll(pair, LANES - 32 * n, 1) for n in range(4)]
    rows = [turned[r % 4][r // 4 : r // 4 + 1] for r in range(count)]
    out[...] = (own + jnp.concatenate(rows, axis=0))[:, :width].astype(jnp.bfloat16)


def shards(
    tokens,
    lengths,
    attn_gain,
    query_weight,
    key_weight,
    value_weight,
    forget_weight,
    forget_offset,
    cache_keys,
    cache_values,
    gate_sum,
    out_weight,
    mlp_gain,
    up_weight,
    down_weight,
):
    rows, cols = tokens.shape
    bf16 = functools.partial(jax.ShapeDtypeStruct, dtype=jnp.bfloat16)
    stack = rows * query_weight.shape[1] // LANES
    line = stack + 16
    far = (
        tokens,
        attn_gain[None, :],
        query_weight,
        key_weight,
        value_weight,
        forget_weight.T,
        lengths[None, :],
        forget_offset[None, :],
    )
    near = [pltpu.VMEM(x.shape, x.dtype) for x in far[:5]]
    x, lengths, forget_offset = call(
        project,
        (
            bf16((RING, line, LANES)),
            jax.ShapeDtypeStruct(far[6].shape, far[6].dtype),
            jax.ShapeDtypeStruct(far[7].shape, far[7].dtype),
        ),
        [HBM] * 8,
        near
        + [
            pltpu.VMEM((forget_weight.shape[1], LANES), jnp.bfloat16),
            pltpu.VMEM((line, LANES), jnp.float32),
            pltpu.SemaphoreType.DMA((8,)),
        ],
    )(*[pltpu.with_memory_space_constraint(x, pltpu.HBM) for x in far])
    x = exchanged(x, ring_groups(True))
    x = call(resend, bf16((RING, line, LANES)), [VMEM])(x)
    x = exchanged(x, ring_groups(False))
    packed = stack + 8
    x = call(attend, bf16((RING, packed, LANES)), [VMEM] * 6)(
        lengths, forget_offset, x, cache_keys, cache_values, gate_sum
    )
    x = exchanged(x, ring_groups(True))
    x = call(combine, bf16((RING, packed, LANES)), [VMEM])(x)
    x = exchanged(x, ring_groups(False))
    group = lax.axis_size(KV_TP)
    x = call(
        finish,
        bf16((group, rows // 2, LANES)),
        [VMEM] * 3,
        [pltpu.VMEM((stack, LANES), jnp.float32)],
    )(x, tokens, out_weight.T)
    x = exchanged(x, None)
    mid, x = call(
        mix,
        (bf16((rows, D)), bf16((2 * group, LANES))),
        [VMEM] * 4,
        [pltpu.VMEM((rows, D), jnp.float32)],
    )(x, mlp_gain[None, :], up_weight, down_weight)
    x = exchanged(x.reshape(group, 2, LANES), None).reshape(2 * group, LANES)
    return call(close, bf16((rows, D // group)), [VMEM, VMEM])(x, mid)


def solution(mesh):
    torus = Mesh(
        mesh.devices.reshape(mesh.shape["dp"], 8, 8, mesh.shape["tp"]), ("dp", "kv_0", "kv_1", "tp")
    )
    placed = (
        P("dp", KV),
        P("dp"),
        P(KV),
        P(KV, "tp"),
        P(KV, "tp"),
        P(KV, "tp"),
        P(),
        P("tp"),
        P("dp", KV, "tp"),
        P("dp", KV, "tp"),
        P("dp", "tp", KV),
        P("tp", KV),
        P(),
        P(None, KV_TP),
        P(KV_TP, None),
    )
    return jax.shard_map(
        shards, mesh=torus, in_specs=placed, out_specs=P("dp", KV_TP), check_vma=False
    )
```

```python
import functools

import jax
import jax.numpy as jnp
from jax import lax
from jax.experimental import pallas as pl
from jax.experimental.pallas import tpu as pltpu
from jax.sharding import Mesh
from jax.sharding import PartitionSpec as P

D = 4096
HEADS = 64
HD = 64
KEY_VALUE_HEADS = 4
KV = ("kv_0", "kv_1")
KV_TP = ("kv_0", "kv_1", "tp")
LANES = 128
HALF = 64
RING = 8
RING_ORDER = (0, 2, 4, 6, 1, 3, 5, 7)

epsilon = 1e-06
floor_score = -1e30

VMEM = pl.BlockSpec(memory_space=pltpu.VMEM)
HBM = pl.BlockSpec(memory_space=pltpu.HBM)


def call(body, out_shape, in_specs, scratch=(), flops=1 << 20):
    return pl.pallas_call(
        body,
        out_shape=out_shape,
        in_specs=in_specs,
        out_specs=jax.tree.map(lambda _: VMEM, out_shape),
        scratch_shapes=scratch,
        compiler_params=pltpu.CompilerParams(vmem_limit_bytes=16 << 20),
        cost_estimate=pl.CostEstimate(flops=flops, bytes_accessed=1 << 20, transcendentals=0),
    )


def lanes_of(shape):
    return lax.broadcasted_iota(jnp.int32, shape, len(shape) - 1)


def rounded(x):
    return x.astype(jnp.bfloat16).astype(jnp.float32)


def exchanged(x, groups):
    return lax.all_to_all(
        x, KV_TP, split_axis=0, concat_axis=0, axis_index_groups=groups, tiled=True
    )


def ring_groups(along_last):
    def member(fixed, moving, core):
        first, last = (fixed, moving) if along_last else (moving, fixed)
        return (first * RING + last) * 2 + core

    return [
        [member(fixed, moving, core) for moving in RING_ORDER]
        for core in range(2)
        for fixed in range(RING)
    ]


def dotted(a, b, b_dim=0):
    return lax.dot_general(
        a, b, (((1,), (b_dim,)), ((), ())), preferred_element_type=jnp.float32
    )


def kv_spot():
    return lax.axis_index("kv_0") * lax.axis_size("kv_1") + lax.axis_index("kv_1")


def project(
    tokens_far, gain_far, query_far, key_far, value_far, forget_far, lengths_far, offsets_far,
    out, lengths, offsets,
    tokens, gain, query_w, key_w, value_w, forget_w, dense, arrived,
):
    spot = kv_spot()
    window = pl.ds(pl.multiple_of((spot // 2) * LANES, LANES), LANES)
    copies = [
        pltpu.make_async_copy(far, near, arrived.at[n])
        for n, (far, near) in enumerate(
            (
                (query_far, query_w),
                (tokens_far, tokens),
                (gain_far, gain),
                (key_far, key_w),
                (value_far, value_w),
                (forget_far.at[:, window], forget_w),
                (lengths_far, lengths),
                (offsets_far, offsets),
            )
        )
    ]
    for copy in copies:
        copy.start()
    for copy in copies[1:3]:
        copy.wait()
    rows = tokens[...].astype(jnp.float32)
    count, cols = rows.shape
    scaled = (rows * gain[...]).astype(jnp.bfloat16)
    wide = scaled.astype(jnp.float32)
    square = jnp.sum(rows * rows, axis=1, keepdims=True)
    square_high = rounded(square)
    for copy in copies[3:]:
        copy.wait()
    gates = forget_w[...].astype(jnp.float32)
    gates = jnp.where(spot % 2 == 0, gates[:, :cols], gates[:, cols:])
    columns = [
        jnp.sum(wide * gates[n : n + 1, :], axis=1, keepdims=True) for n in range(gates.shape[0])
    ] + [square_high, square - square_high]
    lane = lanes_of((count, LANES))
    extra = jnp.zeros(lane.shape, jnp.float32)
    for n, column in enumerate(columns):
        extra = jnp.where((lane == n) | (lane == n + HALF), column, extra)
    third = count // 2
    extra = jnp.where(lane[:third] < HALF, extra[:third], extra[third:])
    copies[0].wait()
    query = dotted(scaled, query_w[...])
    pairs = query.shape[1] // LANES
    stack = pairs * count
    for j in range(pairs):
        dense[pl.ds(j, count, stride=pairs), :] = query[:, LANES * j : LANES * (j + 1)]
    dense[stack : stack + count, :] = dotted(scaled, key_w[...])
    dense[stack + count : stack + 2 * count, :] = dotted(scaled, value_w[...])
    dense[stack + 2 * count : stack + 2 * count + third, :] = extra
    spare = stack + 2 * count + third
    dense[spare:, :] = jnp.zeros((dense.shape[0] - spare, LANES), jnp.float32)
    line = dense[...].astype(jnp.bfloat16)
    for k in range(RING):
        out[k] = line


def summed(parts):
    total = parts[0].astype(jnp.float32)
    for k in range(1, RING):
        total = total + parts[k].astype(jnp.float32)
    return total


def resend(parts, out):
    line = summed(parts).astype(jnp.bfloat16)
    for k in range(RING):
        out[k] = line


def attend(lengths, offsets, parts, keys, values, gate, out):
    count, positions = keys.shape[0], keys.shape[1]
    spot = kv_spot()
    line = summed(parts)
    stack = line.shape[0] - 16
    pairs = stack // count
    tail = line[stack:]
    third = count // 2
    extra = tail[2 * count : 2 * count + third]
    extra = jnp.concatenate((extra, extra), axis=0)
    lane = lanes_of((count, LANES))
    lane = lane - HALF * (lax.broadcasted_iota(jnp.int32, lane.shape, 0) // third)

    def picked(first, last):
        held = jnp.where((lane >= first) & (lane <= last), extra, 0.0)
        return jnp.broadcast_to(jnp.sum(held, axis=1, keepdims=True), lane.shape)

    row_scale = lax.rsqrt(picked(4, 5) / D + epsilon)
    head = 2 * lax.axis_index("tp")
    forget = []
    for n in range(2):
        z = picked(head + n, head + n) * row_scale + offsets[:, n : n + 1]
        forget.append(jnp.minimum(z, 0.0) - jnp.log1p(jnp.exp(-jnp.abs(z))))
    new_key = rounded(tail[:count] * row_scale)
    new_value = rounded(tail[count : 2 * count] * row_scale)
    every = range(count)
    lane = lanes_of((pairs, LANES))
    row = lax.broadcasted_iota(jnp.int32, (pairs, LANES), 0)
    straight = (lane < HALF) == (row < pairs // 2)
    first = spot == 0
    place_of = spot * positions + lanes_of((1, positions))
    live = [place_of < lengths[:, s : s + 1] for s in every]
    both = [rounded(line[pairs * s : pairs * (s + 1)] * row_scale[s : s + 1, :]) for s in every]
    rolled = [pltpu.roll(x, HALF, 1) for x in both]
    queries = [
        jnp.concatenate((jnp.where(straight, x, 0.0), jnp.where(straight, y, 0.0)), axis=0)
        for x, y in zip(both, rolled)
    ]
    scores = [dotted(queries[s].astype(jnp.bfloat16), keys[s], 1) * HD ** (-0.5) for s in every]
    owns = [
        jnp.sum(queries[s] * new_key[s : s + 1, :], axis=1, keepdims=True) * HD ** (-0.5)
        for s in every
    ]
    owns = [jnp.where(first, x, floor_score) for x in owns]
    for s in every:
        lines = [
            jnp.broadcast_to(
                gate[s, n : n + 1, :]
                + jnp.concatenate([forget[n][s : s + 1, :]] * (positions // LANES), axis=1),
                (8, positions),
            )
            for n in range(2)
        ]
        scores[s] = jnp.where(
            live[s], scores[s] + jnp.concatenate(lines + lines, axis=0), floor_score
        )
    tops = [
        rounded(jnp.maximum(jnp.max(scores[s], axis=1, keepdims=True), owns[s])) for s in every
    ]
    weights = [jnp.where(live[s], jnp.exp(scores[s] - tops[s]), 0.0) for s in every]
    own_weights = [jnp.where(first, jnp.exp(owns[s] - tops[s]), 0.0) for s in every]
    mixed = [dotted(weights[s].astype(jnp.bfloat16), values[s]) for s in every]
    totals = [jnp.sum(weights[s], axis=1, keepdims=True) + own_weights[s] for s in every]
    mixed = [mixed[s] + rounded(own_weights[s]) * new_value[s : s + 1, :] for s in every]
    rolled = [pltpu.roll(x[pairs:], HALF, 1) for x in mixed]
    blocks = [
        jnp.where(straight, mixed[s][:pairs], rolled[s]).astype(jnp.bfloat16) for s in every
    ]
    stat_lane = lanes_of((8, LANES))
    stats = jnp.zeros((8, LANES), jnp.float32)
    for s in every:
        total_high = rounded(totals[s])
        for n, column in enumerate((tops[s], total_high, totals[s] - total_high)):
            for g in range(4):
                stats = jnp.where(
                    stat_lane == 32 * g + 8 * n + s, column[8 * g : 8 * g + 8], stats
                )
    blocks.append(stats.astype(jnp.bfloat16))
    line = jnp.concatenate(blocks, axis=0)
    for k in range(RING):
        out[k] = line


def spread(compact, block):
    s, half = divmod(block, 2)
    left, right = (s, 64 + s) if half == 0 else (96 + s, 32 + s)
    source = jnp.where(lanes_of(compact.shape) < HALF, left, right)
    return jnp.take_along_axis(compact, source, axis=1, mode="promise_in_bounds")


def merged(parts):
    rows = parts.shape[1]
    blocks = rows // 8 - 1
    stats = [parts[k, rows - 8 : rows, :].astype(jnp.float32) for k in range(RING)]
    top = functools.reduce(jnp.maximum, stats)
    scales = [jnp.exp(x - top) for x in stats]
    total = functools.reduce(
        jnp.add,
        [
            scale * (pltpu.roll(x, LANES - 8, 1) + pltpu.roll(x, LANES - 16, 1))
            for scale, x in zip(scales, stats)
        ],
    )
    mixed = []
    for b in range(blocks):
        acc = jnp.zeros((8, LANES), jnp.float32)
        for k in range(RING):
            acc = acc + parts[k, 8 * b : 8 * b + 8, :].astype(jnp.float32) * spread(
                scales[k], b
            )
        mixed.append(acc)
    return top, total, mixed


def combine(parts, out):
    top, total, mixed = merged(parts)
    kind = lanes_of((8, LANES)) % 32
    total_high = rounded(total)
    stats = jnp.where(
        kind < 8,
        top,
        jnp.where(
            kind < 16, pltpu.roll(total_high, 8, 1), pltpu.roll(total - total_high, 16, 1)
        ),
    )
    line = jnp.concatenate([x.astype(jnp.bfloat16) for x in mixed + [stats]], axis=0)
    for k in range(RING):
        out[k] = line


def finish(parts, tokens, out_w, out, turned):
    _, total, mixed = merged(parts)
    inverse = 1.0 / total
    for b, acc in enumerate(mixed):
        turned[8 * b : 8 * b + 8, :] = rounded(acc * spread(inverse, b))
    count = tokens.shape[0]
    pairs = turned.shape[0] // count
    attended = jnp.concatenate(
        [turned[pl.ds(j, count, stride=pairs), :] for j in range(pairs)], axis=1
    ).astype(jnp.bfloat16)
    part = dotted(attended, out_w[...], 1)
    part = part + jnp.where(lax.axis_index("tp") == 0, tokens[...].astype(jnp.float32), 0.0)
    third = count // 2
    upper, lower = part[:third], part[third:]
    even = kv_spot() % 2 == 0
    piece = jnp.where(
        even,
        jnp.concatenate((upper, lower), axis=1),
        jnp.concatenate((lower, upper), axis=1),
    ).astype(jnp.bfloat16)
    for k in range(out.shape[0]):
        out[k] = piece


def mix(parts, gain, up_w, down_w, mid_out, out, mid):
    count, width = mid.shape
    third = count // 2
    low = lanes_of((third, LANES)) < HALF
    square = jnp.zeros((count, LANES), jnp.float32)
    for t in range(width // LANES):
        a = rounded(
            parts[4 * t].astype(jnp.float32) + parts[4 * t + 1].astype(jnp.float32)
        )
        b = rounded(
            parts[4 * t + 2].astype(jnp.float32) + parts[4 * t + 3].astype(jnp.float32)
        )
        at = slice(LANES * t, LANES * (t + 1))
        mid[:third, at] = jnp.where(low, a, b)
        mid[third:, at] = pltpu.roll(jnp.where(low, b, a), HALF, 1)
        tile = mid[:, at]
        square = square + tile * tile
    scale = lax.rsqrt(jnp.sum(square, axis=1, keepdims=True) / D + epsilon)
    rows = mid[...]
    mid_out[...] = rows.astype(jnp.bfloat16)
    gained = (rows * gain[...]).astype(jnp.bfloat16)
    hidden = jnp.square(jnp.maximum(dotted(gained, up_w[...]) * scale, 0.0))
    hidden = jnp.concatenate((hidden, jnp.zeros((8 - count, LANES), jnp.float32)), axis=0)
    picked = jnp.concatenate(
        [
            hidden[4 * a + (u + k) % 4 : 4 * a + (u + k) % 4 + 1]
            for k in range(4)
            for u in range(4)
            for a in range(2)
        ],
        axis=0,
    ).astype(jnp.bfloat16)
    spread_out = dotted(picked, down_w[...])
    group = lanes_of((8, LANES)) // 32
    owner = lax.broadcasted_iota(jnp.int32, (8, LANES), 0) // 2
    turn = (group - owner) % 4
    for t in range(width // LANES):
        at = slice(LANES * t, LANES * (t + 1))
        tile = spread_out[:8, at]
        for k in range(1, 4):
            tile = jnp.where(
                turn == k, pltpu.roll(spread_out[8 * k : 8 * k + 8, at], 32 * k, 1), tile
            )
        out[8 * t : 8 * t + 8, :] = tile.astype(jnp.bfloat16)


def close(parts, mid, out):
    total = jnp.zeros((8, LANES), jnp.float32)
    for t in range(parts.shape[0] // 8):
        total = total + parts[8 * t : 8 * t + 8, :].astype(jnp.float32)
    pair = total[0:2] + total[2:4] + total[4:6] + total[6:8]
    count, width = out.shape
    number = kv_spot() * 2 + lax.axis_index("tp")
    tile = mid[:, pl.ds(pl.multiple_of((number // 4) * LANES, LANES), LANES)]
    turn = lax.rem(4 - number % 4, 4) * 32
    own = pltpu.roll(tile.astype(jnp.float32), turn, 1)
    turned = [pair if n == 0 else pltpu.roll(pair, LANES - 32 * n, 1) for n in range(4)]
    rows = [turned[r % 4][r // 4 : r // 4 + 1] for r in range(count)]
    out[...] = (own + jnp.concatenate(rows, axis=0))[:, :width].astype(jnp.bfloat16)


def shards(
    tokens,
    lengths,
    attn_gain,
    query_weight,
    key_weight,
    value_weight,
    forget_weight,
    forget_offset,
    cache_keys,
    cache_values,
    gate_sum,
    out_weight,
    mlp_gain,
    up_weight,
    down_weight,
):
    rows, cols = tokens.shape
    bf16 = functools.partial(jax.ShapeDtypeStruct, dtype=jnp.bfloat16)
    stack = rows * query_weight.shape[1] // LANES
    line = stack + 16
    far = (
        tokens,
        attn_gain[None, :],
        query_weight,
        key_weight,
        value_weight,
        forget_weight.T,
        lengths[None, :],
        forget_offset[None, :],
    )
    near = [pltpu.VMEM(x.shape, x.dtype) for x in far[:5]]
    x, lengths, forget_offset = call(
        project,
        (
            bf16((RING, line, LANES)),
            jax.ShapeDtypeStruct(far[6].shape, far[6].dtype),
            jax.ShapeDtypeStruct(far[7].shape, far[7].dtype),
        ),
        [HBM] * 8,
        near
        + [
            pltpu.VMEM((forget_weight.shape[1], LANES), jnp.bfloat16),
            pltpu.VMEM((line, LANES), jnp.float32),
            pltpu.SemaphoreType.DMA((8,)),
        ],
    )(*[pltpu.with_memory_space_constraint(x, pltpu.HBM) for x in far])
    x = exchanged(x, ring_groups(True))
    x = call(resend, bf16((RING, line, LANES)), [VMEM])(x)
    x = exchanged(x, ring_groups(False))
    packed = stack + 8
    x = call(attend, bf16((RING, packed, LANES)), [VMEM] * 6)(
        lengths, forget_offset, x, cache_keys, cache_values, gate_sum
    )
    x = exchanged(x, ring_groups(False))
    x = call(combine, bf16((RING, packed, LANES)), [VMEM])(x)
    x = exchanged(x, ring_groups(True))
    group = lax.axis_size(KV_TP)
    x = call(
        finish,
        bf16((group, rows // 2, LANES)),
        [VMEM] * 3,
        [pltpu.VMEM((stack, LANES), jnp.float32)],
    )(x, tokens, out_weight.T)
    x = exchanged(x, None)
    mid, x = call(
        mix,
        (bf16((rows, D)), bf16((2 * group, LANES))),
        [VMEM] * 4,
        [pltpu.VMEM((rows, D), jnp.float32)],
    )(x, mlp_gain[None, :], up_weight, down_weight)
    x = exchanged(x.reshape(group, 2, LANES), None).reshape(2 * group, LANES)
    return call(close, bf16((rows, D // group)), [VMEM, VMEM])(x, mid)


def solution(mesh):
    torus = Mesh(
        mesh.devices.reshape(mesh.shape["dp"], 8, 8, mesh.shape["tp"]), ("dp", "kv_0", "kv_1", "tp")
    )
    placed = (
        P("dp", KV),
        P("dp"),
        P(KV),
        P(KV, "tp"),
        P(KV, "tp"),
        P(KV, "tp"),
        P(),
        P("tp"),
        P("dp", KV, "tp"),
        P("dp", KV, "tp"),
        P("dp", "tp", KV),
        P("tp", KV),
        P(),
        P(None, KV_TP),
        P(KV_TP, None),
    )
    return jax.shard_map(
        shards, mesh=torus, in_specs=placed, out_specs=P("dp", KV_TP), check_vma=False
    )
```
